32 devices in a mesh: ep: 8 (over z, x), tp: 4 (over y, core).
Axes of the slice: x: 2, y: 2, z: 4, core: 2. Of those that a mesh axis runs over, the one named last changes fastest.
Arguments:
- queries: bfloat16 [1024, 2048], P('ep', 'tp'), may hold values from -60 to 60
- keys: bfloat16 [1024, 512], P('ep', 'tp'), may hold values from -60 to 60
- values: bfloat16 [1024, 512], P('ep', 'tp'), may hold values from -6 to 6
- cum_gates: float32 [1024, 16], P('ep', 'tp'), may hold values from -259 to 0, as said below
- expert_in: bfloat16 [4096, 4096], P(('ep', 'tp')), may hold values from -6 to 6
- norm_gain: float32 [4096], replicated, may hold values from 0.1 to 1.9
- route_group: int32 [4096, 1], P(('ep', 'tp')), may hold values from 0 to 7; in each aligned block of 128 rows (0 to 127, 128 to 255, ...) at most 24 rows name the same one
- route_member: int32 [4096, 2], P(('ep', 'tp')), may hold values from 0 to 3, all different within a row
- route_weight: float32 [4096, 2], P(('ep', 'tp')), may hold values from 0.1 to 1
- w_gate: bfloat16 [32, 4096, 384], P(('ep', 'tp')), may hold values from -0.09375 to 0.09375
- w_up: bfloat16 [32, 4096, 384], P(('ep', 'tp')), may hold values from -0.09375 to 0.09375
- w_down: bfloat16 [32, 384, 4096], P(('ep', 'tp')), may hold values from -0.3125 to 0.3125
Outputs:
- attended: bfloat16 [1024, 2048], P('ep', 'tp')
- expert_out: bfloat16 [4096, 4096], P(('ep', 'tp'))
The draws below stay inside these ranges and needn't reach their ends.
Inputs may be any that keep to these rules, and one draw needn't show every extreme that they name: `cum_gates`: each head's entries never rise along positions. `route_group`: at most 24 of the rows of one device name one group. `route_member`: the 2 entries of a row differ.
All inputs are finite; a program needn't handle non-finite values.
Results may differ from the reference program's by a relative error of at most 0.0075.
Values may be sent and summed in bfloat16 or wider, within the bound.
A program may use at most 128 MiB of HBM per device.

```python
import math
import jax
import jax.numpy as jnp
import numpy as np
from jax import lax

D = 4096
HEAD_WIDTH = 128
QUERY_HEADS = 16
KEY_VALUE_HEADS = 4
FF = 384
GROUP = 4
TOP = 2
TOK_A = 128
TOK_B = 128
ATTENDED_LENGTH = 1024
TOKENS_B = 4096
CAP = 24
EXPERTS = 32
N_EP = 8
N_TP = 4


def draw_keys(key, part):
    base_value = jax.random.normal(jax.random.fold_in(key, 1), (ATTENDED_LENGTH, KEY_VALUE_HEADS, HEAD_WIDTH), jnp.float32)
    return base_value.reshape(ATTENDED_LENGTH, KEY_VALUE_HEADS * HEAD_WIDTH).astype(jnp.bfloat16)


def draw_queries(key, part):
    heads_per_group = QUERY_HEADS // KEY_VALUE_HEADS
    base_value = jax.random.normal(jax.random.fold_in(key, 2), (ATTENDED_LENGTH, KEY_VALUE_HEADS, heads_per_group, HEAD_WIDTH), jnp.float32)
    return base_value.reshape(ATTENDED_LENGTH, QUERY_HEADS * HEAD_WIDTH).astype(jnp.bfloat16)


def draw_cum_gates(key, part):
    share = 0.5
    slow_heads = jax.random.uniform(jax.random.fold_in(key, 3), (QUERY_HEADS,), jnp.float32) < share
    slow_rate = jnp.exp(jax.random.uniform(jax.random.fold_in(key, 4), (QUERY_HEADS,), jnp.float32, math.log(0.3), 0.0)) / ATTENDED_LENGTH
    fast_rate = 1.0 / jnp.exp(jax.random.uniform(jax.random.fold_in(key, 5), (QUERY_HEADS,), jnp.float32, math.log(30.0), math.log(100.0)))
    rates = jnp.where(slow_heads, slow_rate, fast_rate)
    block_count = ATTENDED_LENGTH // TOK_A
    block_factor = jnp.exp(jax.random.uniform(jax.random.fold_in(key, 6), (block_count,), jnp.float32, math.log(0.5), math.log(2.0)))
    position_factor = jnp.repeat(block_factor, TOK_A)
    roughness = jax.random.uniform(jax.random.fold_in(key, 7), (ATTENDED_LENGTH, QUERY_HEADS), jnp.float32, 0.2, 1.8)
    gate_logarithms = -rates[None, :] * position_factor[:, None] * roughness
    spike_positions = jax.random.randint(jax.random.fold_in(key, 8), (3,), 1, ATTENDED_LENGTH)
    spike_loss = jax.random.uniform(jax.random.fold_in(key, 9), (3, QUERY_HEADS), jnp.float32, 0.2, 0.5)
    spike_values = jnp.zeros((ATTENDED_LENGTH, QUERY_HEADS), jnp.float32).at[spike_positions].add(jnp.log1p(-spike_loss))
    return jnp.cumsum(gate_logarithms + spike_values, axis=0)


def shard_levels(stream_key, dims, pieces, least, largest):
    factor_of, own = 1.0, jax.random.fold_in(stream_key, 6)
    for dim, shards_of in pieces:
        draws = jnp.exp(jax.random.uniform(jax.random.fold_in(own, dim), (shards_of,), jnp.float32, least / len(pieces), largest / len(pieces)))
        factor_of = factor_of * jnp.repeat(draws, dims[dim] // shards_of).reshape([-1 if axis == dim else 1 for axis in range(len(dims))])
    return factor_of


def choose_distinct(key, rows, count, top, lift):
    order = jax.random.permutation(jax.random.fold_in(key, 1), count)
    boost = order
    for power in range(3):
        boost = boost * boost // count
    boost = boost * lift // count
    chance = jax.random.randint(jax.random.fold_in(key, 2), (rows, count), 0, 4096) + boost
    sure = jax.random.permutation(jax.random.fold_in(key, 3), rows)[jnp.arange(count) % rows]
    chance = jnp.where(jnp.arange(rows)[:, None] == sure[None, :], 1 << 14, chance)
    priority = chance * count + jnp.arange(count)
    return lax.top_k(priority.astype(jnp.int32), top)[1].astype(jnp.int32)


def routed_block(own_key, own, number, rows, number_of, top, most, slope):
    sequence = jax.random.permutation(own_key, number_of)
    packed, ordinary = portions_of(number_of, rows * top, most, slope, True), portions_of(number_of, rows * top, most, slope, False)
    places = jnp.arange(number_of)

    def named(sizes, turn):
        used = int((sizes > 0).sum())
        fixed = max(1, used // 4)
        moved = fixed + (places - fixed + turn * (used - fixed)) % max(1, number_of - fixed)
        return jnp.zeros((number_of,), jnp.int32).at[sequence[jnp.where(places < fixed, places, moved)]].set(jnp.asarray(sizes, jnp.int32))

    sizes = jnp.where(number % 4 == 0, named(packed, number // 4), named(ordinary, number - number // 4 - 1))
    mixed = jax.random.permutation(jax.random.fold_in(own, 3), number_of)
    source_of, taker = mixed[0:number_of // 2 * 2:2], mixed[1:number_of // 2 * 2:2]
    margin = jnp.minimum(sizes[source_of] - 1, most - sizes[taker]) // 2
    margin = jnp.where((source_of == sequence[0]) | (taker == sequence[0]) | (sizes[taker] == 0), 0, jnp.maximum(margin, 0))
    moved = jax.random.randint(jax.random.fold_in(own, 4), (number_of // 2,), 0, 1 << 20) % (margin + 1)
    sizes = sizes.at[source_of].add(-moved).at[taker].add(moved)
    items = jnp.searchsorted(jnp.cumsum(sizes), jnp.arange(rows * top), side="right").astype(jnp.int32)
    grid = items.reshape(top, rows).T
    grid = grid[jax.random.permutation(jax.random.fold_in(own, 1), rows)]
    turn = jax.random.randint(jax.random.fold_in(own, 2), (rows, 1), 0, top)
    return jnp.take_along_axis(grid, (jnp.arange(top)[None, :] + turn) % top, axis=1)


def portions_of(count, total, reach, slope, full):
    portions = [(1 << 20) // math.isqrt(rank ** slope) + 1 for rank in range(1, count + 1)]
    largest = reach if full else min(reach, max(-(-total // count), total * portions[0] // sum(portions)))
    least = 1 if total - largest >= count - 1 else 0
    holding, spare = [largest] + [least] * (count - 1), total - largest - least * (count - 1)
    while spare > 0:
        candidates = [i for i in range(1, count) if holding[i] < largest] or [i for i in range(1, count) if holding[i] < reach]
        pool, left = sum([portions[i] for i in candidates]), spare
        for i in candidates:
            extra = min(reach - holding[i], max(1, left * portions[i] // pool), spare)
            holding[i] = holding[i] + extra
            spare = spare - extra
    return np.array(holding)


def scatter_about(own_key, shape, scale, bound, cuts=(), held_as=jnp.bfloat16):
    level = shard_levels(own_key, shape, cuts, -0.22, 0.18) if cuts else 1.0
    drawn = jax.random.normal(own_key, shape, jnp.float32) * scale * level
    return jnp.minimum(jnp.maximum(drawn, -bound), bound).astype(held_as)


def setup_inputs(seed: int = 0) -> dict:
    seeds = jax.random.split(jax.random.key(seed), 13)
    queries = draw_queries(jax.random.fold_in(seeds[12], 71), 0)
    keys = draw_keys(jax.random.fold_in(seeds[12], 71), 0)
    values = scatter_about(seeds[2], (ATTENDED_LENGTH, KEY_VALUE_HEADS * HEAD_WIDTH), 1.0, 6.0, ((0, 8), (1, 4)))
    cum_gates = draw_cum_gates(jax.random.fold_in(seeds[12], 71), 0)
    expert_in = scatter_about(seeds[4], (TOKENS_B, D), 1.0, 6.0, ((0, 32),))
    norm_gain = jnp.clip(1.0 + 0.18 * jax.random.normal(seeds[5], (D,), jnp.float32), 0.1, 1.9)
    route_group_keys = jax.random.split(jax.random.fold_in(seeds[6], 1), TOKENS_B // TOK_B)
    route_group_turns = jax.random.permutation(jax.random.fold_in(seeds[6], 3), TOKENS_B // TOK_B)
    route_group = jax.vmap(lambda own, number: routed_block(jax.random.fold_in(seeds[6], 2), own, number, TOK_B, N_EP, 1, CAP, 2))(route_group_keys, route_group_turns).reshape((TOKENS_B, 1))
    route_member = choose_distinct(seeds[7], TOKENS_B, GROUP, TOP, 0)
    route_weight = jnp.clip(jnp.exp(math.log(1.0) - 2.3025851 * jax.random.uniform(seeds[8], (TOKENS_B, TOP), jnp.float32) ** shard_levels(seeds[8], (TOKENS_B, TOP), ((0, 32),), -0.2, 0.2)), 0.1, 1.0)
    w_gate = scatter_about(seeds[9], (EXPERTS, D, FF), D ** -0.5, 0.09375, ((0, 32),))
    w_up = scatter_about(seeds[10], (EXPERTS, D, FF), D ** -0.5, 0.09375, ((0, 32),))
    w_down = scatter_about(seeds[11], (EXPERTS, FF, D), FF ** -0.5, 0.3125, ((0, 32),))
    return {"queries": queries, "keys": keys, "values": values, "cum_gates": cum_gates, "expert_in": expert_in, "norm_gain": norm_gain, "route_group": route_group, "route_member": route_member, "route_weight": route_weight, "w_gate": w_gate, "w_up": w_up, "w_down": w_down}


NEGATIVE = -1e+30
EPSILON = 1e-06

def attention_part(queries, keys, values, cum_gates):
    sequence_length = queries.shape[0]
    heads_per_group = QUERY_HEADS // KEY_VALUE_HEADS
    rows_per_block = math.gcd(sequence_length, 512)
    score_scale = HEAD_WIDTH ** (-0.5)
    every_query = queries.reshape(sequence_length, KEY_VALUE_HEADS, heads_per_group, HEAD_WIDTH).astype(jnp.float32)
    every_key = keys.reshape(sequence_length, KEY_VALUE_HEADS, HEAD_WIDTH).astype(jnp.float32)
    every_value = values.reshape(sequence_length, KEY_VALUE_HEADS, HEAD_WIDTH).astype(jnp.float32)

    def query_block(block_index):
        start_row = block_index * rows_per_block
        query_rows = lax.dynamic_slice_in_dim(every_query, start_row, rows_per_block, 0)
        query_gates = lax.dynamic_slice_in_dim(cum_gates, start_row, rows_per_block, 0)
        query_pos = start_row + jnp.arange(rows_per_block, dtype=jnp.int32)

        def key_step(key_index, carried):
            running, totals, accumulated = carried
            key_start = (key_index * rows_per_block).astype(jnp.int32)
            key_rows = lax.dynamic_slice_in_dim(every_key, key_start, rows_per_block, 0)
            rows_of_value = lax.dynamic_slice_in_dim(every_value, key_start, rows_per_block, 0)
            key_gates = lax.dynamic_slice_in_dim(cum_gates, key_start, rows_per_block, 0)
            key_pos = key_start + jnp.arange(rows_per_block, dtype=jnp.int32)
            scores = jnp.einsum('qgrd,kgd->grqk', query_rows, key_rows).reshape(QUERY_HEADS, rows_per_block, rows_per_block) * score_scale
            scores = scores + query_gates.T[:, :, None] - key_gates.T[:, None, :]
            allowed = (key_pos[None, :] <= query_pos[:, None])[None]
            scores = jnp.where(allowed, scores, NEGATIVE)
            new_max = jnp.maximum(running, lax.optimization_barrier(jnp.max(scores, axis=-1)))
            weights = jnp.where(allowed, jnp.exp(scores - new_max[..., None]), 0.0)
            factor = jnp.exp(running - new_max)
            totals = totals * factor + lax.optimization_barrier(jnp.sum(weights, axis=-1))
            rounded_count = lax.optimization_barrier(weights.astype(jnp.bfloat16)).astype(jnp.float32)
            inner_product = jnp.einsum('tjub,btl->tjul', rounded_count.reshape(KEY_VALUE_HEADS, heads_per_group, rows_per_block, rows_per_block), rows_of_value)
            accumulated = accumulated * factor[..., None] + inner_product.reshape(QUERY_HEADS, rows_per_block, HEAD_WIDTH)
            return (new_max, totals, accumulated)
        initial = (jnp.full((QUERY_HEADS, rows_per_block), NEGATIVE, jnp.float32), jnp.zeros((QUERY_HEADS, rows_per_block), jnp.float32), jnp.zeros((QUERY_HEADS, rows_per_block, HEAD_WIDTH), jnp.float32))
        running, totals, accumulated = lax.fori_loop(0, block_index + 1, key_step, initial)
        result = accumulated / totals[..., None]
        return jnp.transpose(result, (1, 0, 2)).reshape(rows_per_block, QUERY_HEADS * HEAD_WIDTH).astype(jnp.bfloat16)
    blocks = lax.map(query_block, jnp.arange(sequence_length // rows_per_block, dtype=jnp.int32))
    return blocks.reshape(sequence_length, QUERY_HEADS * HEAD_WIDTH)

def expert_part(expert_in, norm_gain, route_group, route_member, route_weight, w_gate, w_up, w_down):
    count_rows, model_width = expert_in.shape
    floats = expert_in.astype(jnp.float32)
    normed = (floats * lax.rsqrt(lax.optimization_barrier(jnp.mean(floats * floats, axis=-1, keepdims=True)) + EPSILON) * norm_gain).astype(jnp.bfloat16)
    members = jnp.arange(GROUP, dtype=jnp.int32)
    mix_weights = jnp.zeros((count_rows, GROUP), jnp.float32)
    for rank_index in range(TOP):
        mix_weights = mix_weights + route_weight[:, rank_index:rank_index + 1] * (route_member[:, rank_index:rank_index + 1] == members[None, :]).astype(jnp.float32)
    mix_weights = lax.optimization_barrier(mix_weights.astype(jnp.bfloat16)).astype(jnp.float32)
    group_ids = route_group[:, 0]
    group_match = (group_ids[:, None] == jnp.arange(N_EP, dtype=jnp.int32)[None, :]).astype(jnp.int32)
    rank_within = lax.optimization_barrier(jnp.sum((jnp.cumsum(group_match, axis=0) - group_match) * group_match, axis=1)).astype(jnp.int32)
    slots_per_group = CAP * N_EP * N_TP
    row_table = jnp.full((N_EP, slots_per_group), count_rows, jnp.int32).at[group_ids, rank_within].set(jnp.arange(count_rows, dtype=jnp.int32))
    padded_rows = jnp.concatenate([normed, jnp.zeros((1, model_width), jnp.bfloat16)], axis=0)
    padded_weights = jnp.concatenate([mix_weights, jnp.zeros((1, GROUP), jnp.float32)], axis=0)

    def one_group(group_index):
        row_index = row_table[group_index]
        rows_in = padded_rows[row_index]
        weights_in = padded_weights[row_index]
        combined = jnp.zeros((slots_per_group, model_width), jnp.float32)
        for member in range(GROUP):
            expert_index = group_index * GROUP + member
            gate_part = jnp.dot(rows_in, w_gate[expert_index], preferred_element_type=jnp.float32)
            up_part = jnp.dot(rows_in, w_up[expert_index], preferred_element_type=jnp.float32)
            hidden = (jax.nn.silu(gate_part) * up_part).astype(jnp.bfloat16)
            outputs = jnp.dot(hidden, w_down[expert_index], preferred_element_type=jnp.float32).astype(jnp.bfloat16)
            combined = combined + weights_in[:, member:member + 1] * outputs.astype(jnp.float32)
        return combined.astype(jnp.bfloat16)
    results = lax.map(one_group, jnp.arange(N_EP, dtype=jnp.int32))
    table_out = jnp.zeros((count_rows + 1, model_width), jnp.bfloat16).at[row_table.reshape(-1)].set(results.reshape(-1, model_width))
    return table_out[:count_rows]

def reference(queries, keys, values, cum_gates, expert_in, norm_gain, route_group, route_member, route_weight, w_gate, w_up, w_down):
    attended = attention_part(queries, keys, values, cum_gates)
    expert_out = expert_part(expert_in, norm_gain, route_group, route_member, route_weight, w_gate, w_up, w_down)
    return (attended, expert_out)
```

```python
import functools
import itertools
import math

import jax
import jax.numpy as jnp
from jax import lax
from jax.experimental import pallas as pl
from jax.experimental.pallas import tpu as pltpu
from jax.sharding import PartitionSpec as P

HEAD_WIDTH = 128
GROUP = 4
TOP = 2


OUTER, INNER, BOTH = range(3)
ARRIVE, CROSS, COMPUTE, CORE_SUM, CHIP, FINAL, KEYS, WEIGHTS = range(8)
HALVES = 2
CHUNKS = ((4, 5), (6, 7), (2, 3), (0, 1))
DISPATCH = ((6, 4, 5, 2, 1, 7, 3), (6, 4, 5, 2, 1, 7, 3))
PLAN = (
    (BOTH, ARRIVE, 0, 1),
    (BOTH, ARRIVE, 0, 0),
    (BOTH, ARRIVE, 1, 0),
    (BOTH, ARRIVE, 1, 1),
    (OUTER, ARRIVE, 6, 1),
    (OUTER, ARRIVE, 2, 1),
    (INNER, ARRIVE, 4, 0),
    (INNER, ARRIVE, 4, 1),
    (INNER, ARRIVE, 5, 0),
    (INNER, ARRIVE, 5, 1),
    (INNER, CROSS, 4, 1),
    (BOTH, CROSS, 0, 1),
    (OUTER, CROSS, 1, 0),
    (INNER, ARRIVE, 2, 0),
    (INNER, CROSS, 4, 0),
    (INNER, CROSS, 0, 0),
    (INNER, CROSS, 5, 1),
    (INNER, CROSS, 5, 0),
    (BOTH, ARRIVE, 6, 0),
    (INNER, ARRIVE, 2, 1),
    (INNER, ARRIVE, 6, 1),
    (INNER, WEIGHTS, 0, 0),
    (INNER, COMPUTE, 0, 0),
    (INNER, CROSS, 1, 1),
    (INNER, CORE_SUM, 0, 0),
    (INNER, CROSS, 2, 0),
    (INNER, CROSS, 2, 1),
    (INNER, CHIP, 4, 0),
    (BOTH, ARRIVE, 3, 0),
    (INNER, CROSS, 1, 0),
    (BOTH, ARRIVE, 3, 1),
    (OUTER, CROSS, 0, 0),
    (OUTER, CROSS, 2, 1),
    (OUTER, CROSS, 6, 1),
    (OUTER, ARRIVE, 2, 0),
    (OUTER, CROSS, 1, 1),
    (BOTH, CROSS, 6, 0),
    (OUTER, WEIGHTS, 0, 0),
    (INNER, CORE_SUM, 0, 1),
    (INNER, FINAL, 4, 0),
    (INNER, CROSS, 6, 1),
    (INNER, CHIP, 5, 1),
    (INNER, CHIP, 4, 1),
    (BOTH, COMPUTE, 3, 0),
    (OUTER, ARRIVE, 7, 0),
    (OUTER, CROSS, 3, 1),
    (BOTH, ARRIVE, 7, 1),
    (OUTER, ARRIVE, 4, 0),
    (OUTER, CROSS, 7, 0),
    (OUTER, ARRIVE, 4, 1),
    (OUTER, CROSS, 7, 1),
    (INNER, FINAL, 5, 1),
    (INNER, CHIP, 5, 0),
    (INNER, CROSS, 3, 0),
    (INNER, CROSS, 3, 1),
    (INNER, ARRIVE, 7, 0),
    (INNER, CORE_SUM, 3, 1),
    (INNER, COMPUTE, 2, 0),
    (BOTH, CORE_SUM, 3, 0),
    (OUTER, CROSS, 3, 0),
    (OUTER, ARRIVE, 5, 0),
    (INNER, CORE_SUM, 2, 1),
    (INNER, CROSS, 7, 1),
    (INNER, FINAL, 4, 1),
    (INNER, CHIP, 1, 1),
    (INNER, CHIP, 1, 0),
    (INNER, CROSS, 7, 0),
    (INNER, CORE_SUM, 2, 0),
    (INNER, CHIP, 3, 1),
    (INNER, KEYS, 4, 0),
    (BOTH, COMPUTE, 1, 0),
    (OUTER, ARRIVE, 5, 1),
    (OUTER, CROSS, 2, 0),
    (OUTER, CORE_SUM, 1, 1),
    (BOTH, CORE_SUM, 1, 0),
    (OUTER, CHIP, 6, 0),
    (OUTER, CHIP, 7, 1),
    (OUTER, COMPUTE, 2, 0),
    (OUTER, CORE_SUM, 2, 0),
    (OUTER, CROSS, 5, 1),
    (OUTER, CROSS, 4, 1),
    (OUTER, CROSS, 5, 0),
    (OUTER, CHIP, 6, 1),
    (OUTER, CHIP, 7, 0),
    (OUTER, CROSS, 4, 0),
    (OUTER, FINAL, 6, 0),
    (OUTER, COMPUTE, 0, 0),
    (OUTER, CORE_SUM, 2, 1),
    (OUTER, CORE_SUM, 0, 1),
    (OUTER, CHIP, 5, 1),
    (OUTER, CORE_SUM, 0, 0),
    (OUTER, FINAL, 6, 1),
    (OUTER, CHIP, 5, 0),
    (OUTER, CHIP, 4, 1),
    (OUTER, FINAL, 7, 1),
    (OUTER, CHIP, 3, 1),
    (OUTER, CHIP, 4, 0),
    (OUTER, CHIP, 1, 0),
    (OUTER, CORE_SUM, 3, 1),
    (OUTER, KEYS, 4, 0),
    (OUTER, FINAL, 7, 0),
    (OUTER, FINAL, 5, 1),
    (INNER, FINAL, 1, 1),
    (INNER, CHIP, 3, 0),
    (BOTH, FINAL, 5, 0),
    (OUTER, FINAL, 4, 1),
    (OUTER, CHIP, 2, 0),
    (OUTER, CHIP, 2, 1),
    (BOTH, FINAL, 3, 1),
    (OUTER, FINAL, 4, 0),
    (OUTER, CHIP, 1, 1),
    (INNER, CHIP, 2, 0),
    (INNER, CORE_SUM, 1, 1),
    (INNER, CHIP, 2, 1),
    (INNER, CHIP, 7, 0),
    (INNER, CHIP, 7, 1),
    (INNER, FINAL, 3, 0),
    (INNER, CHIP, 6, 1),
    (INNER, CHIP, 6, 0),
    (INNER, CHIP, 0, 0),
    (BOTH, KEYS, 2, 0),
    (INNER, FINAL, 7, 0),
    (INNER, FINAL, 7, 1),
    (INNER, FINAL, 6, 1),
    (INNER, FINAL, 2, 0),
    (BOTH, FINAL, 1, 0),
    (OUTER, CHIP, 3, 0),
    (OUTER, CHIP, 0, 1),
    (INNER, FINAL, 6, 0),
    (BOTH, FINAL, 2, 1),
    (OUTER, CHIP, 0, 0),
    (OUTER, FINAL, 2, 0),
    (OUTER, FINAL, 3, 0),
    (OUTER, FINAL, 1, 1),
    (OUTER, FINAL, 0, 1),
    (INNER, CHIP, 0, 1),
    (BOTH, FINAL, 0, 0),
    (INNER, FINAL, 0, 1),
)


NEGATIVE = -1e30
EPSILON = 1e-06


def group_fold(states, prepared_group, key_piece, value_piece, start_row, all_gates, key_heads):
    query_rows, query_pos, query_gates = prepared_group
    count_queries = query_rows.shape[0]
    head_count = all_gates.shape[1]
    heads_per_group = head_count // key_heads
    piece_rows = key_piece.shape[0]
    rows_per_block = math.gcd(piece_rows, 512)
    score_scale = HEAD_WIDTH ** (-0.5)

    def key_step(step_index, carried):
        running, totals, accumulated = carried
        offset = step_index * rows_per_block
        key_rows = lax.dynamic_slice_in_dim(key_piece, offset, rows_per_block, 0).reshape(
            rows_per_block, key_heads, HEAD_WIDTH
        )
        rows_of_value = lax.dynamic_slice_in_dim(value_piece, offset, rows_per_block, 0).reshape(
            rows_per_block, key_heads, HEAD_WIDTH
        )
        key_gates = lax.dynamic_slice_in_dim(all_gates, offset, rows_per_block, 0)
        key_pos = offset + jnp.arange(rows_per_block, dtype=jnp.int32)
        scores = jnp.einsum(
            "qgrd,kgd->grqk", query_rows, key_rows, preferred_element_type=jnp.float32
        )
        scores = scores.reshape(head_count, count_queries, rows_per_block) * score_scale
        scores = scores + query_gates.T[:, :, None] - key_gates.T[:, None, :]
        allowed = (key_pos[None, :] <= query_pos[:, None])[None]
        scores = jnp.where(allowed, scores, NEGATIVE)
        new_max = jnp.maximum(running, jnp.max(scores, axis=-1))
        weights = jnp.where(allowed, jnp.exp(scores - new_max[..., None]), 0.0)
        factor = jnp.exp(running - new_max)
        totals = totals * factor + jnp.sum(weights, axis=-1)
        inner_product = jnp.einsum(
            "tjub,btl->tjul",
            weights.astype(jnp.bfloat16).reshape(
                key_heads, heads_per_group, count_queries, rows_per_block
            ),
            rows_of_value,
            preferred_element_type=jnp.float32,
        )
        accumulated = accumulated * factor[..., None] + inner_product.reshape(
            head_count, count_queries, HEAD_WIDTH
        )
        return (new_max, totals, accumulated)

    def run_all(carried):
        return lax.fori_loop(0, piece_rows // rows_per_block, key_step, carried)

    def keep_state(carried):
        return carried

    return lax.cond(start_row <= query_pos[-1], run_all, keep_state, states)


def fold_attention(groups, keys, values, all_gates):
    key_heads = keys.shape[1] // HEAD_WIDTH
    head_count = all_gates.shape[1]
    prepared = []
    initial = []
    for query_block, query_pos in groups:
        count_queries = query_block.shape[0]
        prepared.append(
            (
                query_block.reshape(count_queries, key_heads, head_count // key_heads, HEAD_WIDTH),
                query_pos,
                all_gates[query_pos],
            )
        )
        initial.append(
            (
                jnp.full((head_count, count_queries), NEGATIVE, jnp.float32),
                jnp.zeros((head_count, count_queries), jnp.float32),
                jnp.zeros((head_count, count_queries, HEAD_WIDTH), jnp.float32),
            )
        )
    carried = tuple(initial)
    start_row = jnp.int32(0)
    key_piece = lax.all_gather(keys, "ep", axis=0, tiled=True)
    value_piece = lax.all_gather(values, "ep", axis=0, tiled=True)
    finals = tuple(
        (
            group_fold(
                states, prepared_group, key_piece, value_piece, start_row, all_gates, key_heads
            )
            for states, prepared_group in zip(carried, prepared)
        )
    )
    outputs = []
    for running, totals, accumulated in finals:
        result = accumulated / totals[..., None]
        outputs.append(
            jnp.transpose(result, (1, 0, 2))
            .reshape(result.shape[1], head_count * HEAD_WIDTH)
            .astype(jnp.bfloat16)
        )
    return outputs


def attention_half(queries, keys, values, cum_gates):
    count_rows = queries.shape[0]
    head_count = cum_gates.shape[1]
    ep_index = lax.axis_index("ep")
    all_gates = lax.all_gather(cum_gates, "ep", axis=0, tiled=True)
    query_heads = queries.reshape(count_rows, head_count, HEAD_WIDTH)
    positions = ep_index * count_rows + jnp.arange(count_rows, dtype=jnp.int32)
    outputs = fold_attention([(query_heads, positions)], keys, values, all_gates)
    attended = outputs[0]
    return attended


def expert_half(
    expert_in, norm_gain, route_group, route_member, route_weight, w_gate, w_up, w_down
):
    count_rows, model_width = expert_in.shape
    ep_size = lax.axis_size("ep")
    tp_size = lax.axis_size("tp")
    capacity = max(2, (3 * count_rows + 2 * ep_size - 1) // (2 * ep_size))
    floats = expert_in.astype(jnp.float32)
    normed = (
        floats * lax.rsqrt(jnp.mean(floats * floats, axis=-1, keepdims=True) + EPSILON) * norm_gain
    ).astype(jnp.bfloat16)
    members = jnp.arange(GROUP, dtype=jnp.int32)
    mix_weights = jnp.zeros((count_rows, GROUP), jnp.float32)
    for rank_index in range(TOP):
        mix_weights = mix_weights + route_weight[:, rank_index : rank_index + 1] * (
            route_member[:, rank_index : rank_index + 1] == members[None, :]
        ).astype(jnp.float32)
    mix_weights = mix_weights.astype(jnp.bfloat16)
    group_ids = route_group[:, 0]
    group_match = (group_ids[:, None] == jnp.arange(ep_size, dtype=jnp.int32)[None, :]).astype(
        jnp.int32
    )
    rank_within = jnp.sum((jnp.cumsum(group_match, axis=0) - group_match) * group_match, axis=1)
    slot_of_row = group_ids * capacity + rank_within
    row_of_slot = (
        jnp.full((ep_size * capacity,), count_rows, jnp.int32)
        .at[slot_of_row]
        .set(jnp.arange(count_rows, dtype=jnp.int32))
    )
    padded_rows = jnp.concatenate([normed, jnp.zeros((1, model_width), jnp.bfloat16)], axis=0)
    padded_weights = jnp.concatenate([mix_weights, jnp.zeros((1, GROUP), jnp.bfloat16)], axis=0)
    send_rows = padded_rows[row_of_slot].reshape(ep_size, capacity, model_width)
    send_weights = padded_weights[row_of_slot].reshape(ep_size, capacity, GROUP)
    gate_matrix = w_gate[0]
    up_matrix = w_up[0]
    down_matrix = w_down[0]
    arrived_rows = lax.all_to_all(send_rows, "ep", split_axis=0, concat_axis=0, tiled=True)
    arrived_weights = lax.all_to_all(send_weights, "ep", split_axis=0, concat_axis=0, tiled=True)
    sources = arrived_rows.shape[0]
    per_source = arrived_rows.shape[1]
    flat_rows = arrived_rows.reshape(sources * per_source, model_width)
    pieces = lax.all_gather(flat_rows, "tp", axis=0, tiled=True)
    gate_part = jnp.dot(pieces, gate_matrix, preferred_element_type=jnp.float32)
    up_part = jnp.dot(pieces, up_matrix, preferred_element_type=jnp.float32)
    hidden = (jax.nn.silu(gate_part) * up_part).astype(jnp.bfloat16)
    expert_outputs = jnp.dot(hidden, down_matrix, preferred_element_type=jnp.float32).astype(
        jnp.bfloat16
    )
    member_outputs = lax.all_to_all(
        expert_outputs.reshape(tp_size, sources * per_source, model_width),
        "tp",
        split_axis=0,
        concat_axis=0,
        tiled=True,
    )
    flat_weights = arrived_weights.reshape(sources * per_source, GROUP).astype(jnp.float32)
    combined = jnp.zeros((sources * per_source, model_width), jnp.float32)
    for member in range(GROUP):
        combined = combined + flat_weights[:, member : member + 1] * member_outputs[member]
    mixed = combined.astype(jnp.bfloat16).reshape(sources, per_source, model_width)
    returned = lax.all_to_all(mixed, "ep", split_axis=0, concat_axis=0, tiled=True)
    return returned.reshape(ep_size * capacity, model_width)[slot_of_row]


def flipped(index, bits):
    result = index
    place = 1
    while place <= bits:
        if bits & place:
            result = result + place - 2 * place * ((index // place) % 2)
        place = place * 2
    return result


def fused_kernel(
    n,
    capacity,
    queries_in,
    keys_in,
    values_in,
    gates_in,
    expert_rows,
    gain_in,
    route_group_in,
    route_member_in,
    route_weight_in,
    w_gate,
    w_up,
    w_down,
    attended_out,
    expert_result,
    queries,
    keys,
    values,
    gates,
    expert_in,
    gain,
    route_group,
    route_member,
    route_weight,
    attended,
    expert_out,
    input_sem,
    output_sem,
    send,
    pieces,
    gate_up,
    down,
    partial,
    from_core,
    to_chip,
    from_chip,
    final,
    returned,
    all_keys,
    all_values,
    own_gates,
    all_gates,
    weight_sem,
    disp_send,
    disp_recv,
    fwd_send,
    fwd_recv,
    core_send,
    core_recv,
    chip_send,
    chip_recv,
    ret_send,
    ret_recv,
    key_send,
    key_recv,
):
    f32, bf16 = jnp.float32, jnp.bfloat16
    rows, width = expert_in.shape
    hidden_width = down.shape[0]
    wide = pieces.shape[-1]
    me = lax.axis_index("ep")
    mine = lax.axis_index("tp")
    core = mine % 2
    side = mine // 2
    twin = flipped(mine, 1)
    across = flipped(mine, 2)
    diagonal = flipped(mine, 3)

    inputs = (
        (route_group_in, route_group),
        (route_member_in, route_member),
        (route_weight_in, route_weight),
        (expert_rows, expert_in),
        (gain_in, gain),
        (keys_in, keys),
        (values_in, values),
        (gates_in, gates),
        (queries_in, queries),
    )
    input_copies = [
        pltpu.make_async_copy(source, target, input_sem.at[index])
        for index, (source, target) in enumerate(inputs)
    ]
    weight_copies = [
        pltpu.make_async_copy(w_gate.at[0], gate_up.at[:, pl.ds(0, hidden_width)], weight_sem.at[0]),
        pltpu.make_async_copy(
            w_up.at[0], gate_up.at[:, pl.ds(hidden_width, hidden_width)], weight_sem.at[1]
        ),
        pltpu.make_async_copy(w_down.at[0], down, weight_sem.at[2]),
    ]
    for copy in input_copies:
        copy.start()

    def has(index, bit):
        return (index // bit) % 2 == 1

    barrier = pltpu.get_barrier_semaphore()

    def remote(source, target, send_sem, recv_sem, ep, tp):
        return pltpu.make_async_remote_copy(
            src_ref=source,
            dst_ref=target,
            send_sem=send_sem,
            recv_sem=recv_sem,
            device_id={"ep": ep, "tp": tp},
            device_id_type=pl.DeviceIdType.MESH,
        )

    for step in range(1, n):
        pl.semaphore_signal(
            barrier,
            inc=1,
            device_id={"ep": flipped(me, step), "tp": mine},
            device_id_type=pl.DeviceIdType.MESH,
        )
    for other in (twin, across):
        pl.semaphore_signal(
            barrier,
            inc=1,
            device_id={"ep": me, "tp": other},
            device_id_type=pl.DeviceIdType.MESH,
        )

    for copy in weight_copies:
        copy.start()
    for copy in input_copies[:3]:
        copy.wait()

    lanes = lax.broadcasted_iota(jnp.int32, (rows, 128), 1)
    row_i = lax.broadcasted_iota(jnp.int32, (rows, rows), 0)
    col_i = lax.broadcasted_iota(jnp.int32, (rows, rows), 1)
    earlier = (col_i < row_i).astype(bf16)
    same = row_i == col_i

    def column(row):
        return jnp.sum(jnp.where(same, row.astype(f32), 0.0), axis=1, keepdims=True)

    group = column(route_group[...])
    match = (group == lanes.astype(f32)).astype(f32)
    ranks = jnp.dot(earlier, match.astype(bf16), preferred_element_type=f32)
    rank_within = jnp.sum(ranks * match, axis=1, keepdims=True)
    slot = group * float(capacity) + rank_within
    slot_row = jnp.sum(jnp.where(same, slot, 0.0), axis=0, keepdims=True)
    slots = n * capacity
    place = (
        lax.broadcasted_iota(jnp.int32, (slots, rows), 0).astype(f32) == slot_row
    ).astype(f32).astype(bf16)
    mix = jnp.zeros((rows, 128), f32)
    for rank_index in range(TOP):
        mix = mix + jnp.where(
            column(route_member[rank_index : rank_index + 1, :]) == lanes.astype(f32),
            column(route_weight[rank_index : rank_index + 1, :]),
            0.0,
        )
    for copy in input_copies[3:5]:
        copy.wait()
    floats = expert_in[...].astype(f32)
    scale = lax.rsqrt(jnp.mean(floats * floats, axis=-1, keepdims=True) + EPSILON)
    normed = (floats * scale * gain[...]).astype(bf16)
    send[:, :, pl.ds(0, width)] = (
        jnp.dot(place, normed, preferred_element_type=f32)
        .astype(bf16)
        .reshape(n, capacity, width)
    )
    send[:, :, pl.ds(width, wide - width)] = (
        jnp.dot(place, mix.astype(bf16), preferred_element_type=f32)
        .astype(bf16)
        .reshape(n, capacity, wide - width)
    )
    for copy in input_copies[5:]:
        copy.wait()
    heads = gates.shape[0]
    own_gates[pl.ds(0, heads), :] = gates[...]
    for flip in range(1, n):

        @pl.when(jnp.logical_not(has(me, 1 << (flip.bit_length() - 1))))
        def _():
            block = flipped(me, flip)
            all_keys[block] = jnp.zeros_like(all_keys[block])
            all_values[block] = jnp.zeros_like(all_values[block])
            all_gates[block] = jnp.zeros_like(all_gates[block])

    all_gates[me] = own_gates[...]
    all_keys[me] = keys[...]
    all_values[me] = values[...]

    pl.semaphore_wait(barrier, n + 1)

    half = width // HALVES
    inner = ((me // 2 + 1) // 2) % 2

    def columns(part):
        return pl.ds(part * half, half + (wide - width if part == HALVES - 1 else 0))

    def narrow(part):
        return pl.ds(part * half, half)

    def dispatch(peer, part):
        return remote(
            send.at[peer, :, columns(part)],
            pieces.at[mine, me, :, columns(part)],
            disp_send.at[peer, part],
            disp_recv.at[me, part],
            peer,
            mine,
        )

    def arrival(peer, part):
        return remote(
            send.at[peer, :, columns(part)],
            pieces.at[mine, peer, :, columns(part)],
            disp_send.at[peer, part],
            disp_recv.at[peer, part],
            peer,
            mine,
        )

    def send_rows(order):
        for step in order:
            for part in range(HALVES):
                dispatch(flipped(me, step), part).start()

    if DISPATCH[0] == DISPATCH[1]:
        send_rows(DISPATCH[0])
    else:
        for kind in range(2):
            pl.when(inner == kind)(functools.partial(send_rows, DISPATCH[kind]))
    pieces[mine, me] = send[me]

    shared = (all_keys, all_values, all_gates)

    bits = [1 << power for power in reversed(range((n - 1).bit_length()))]

    def high(number):
        return 1 << (number.bit_length() - 1)

    def key_send_copy(which, bit, others):
        block = shared[which].at[flipped(me, others)]
        flip = others | bit
        return remote(
            block,
            block,
            key_send.at[which, flip],
            key_recv.at[which, flip],
            flipped(me, bit),
            mine,
        )

    def key_arrival(which, flip):
        block = shared[which].at[flipped(me, flip)]
        return remote(
            block, block, key_send.at[which, flip], key_recv.at[which, flip], me, mine
        )

    def key_flips(bit):
        return [others for others in range(0, n, 2 * bit)]

    def sends_keys(bit, others):
        return has(me, high(others)) if others else jnp.logical_not(has(me, bit))

    def wait_keys(bit):
        for others in key_flips(bit):
            flip = others | bit

            @pl.when(has(me, high(flip)))
            def _():
                for which in range(3):
                    key_arrival(which, flip).wait_recv()

    def start_keys(bit):
        for others in key_flips(bit):

            @pl.when(sends_keys(bit, others))
            def _():
                for which in range(3):
                    key_send_copy(which, bit, others).start()

    def pair_of(chunk):
        steps = CHUNKS[chunk]
        if len(steps) == 1:
            return pl.ds(flipped(me, steps[0]), 1)
        return pl.ds(flipped(me // 2, steps[0] // 2) * 2, 2)

    def forward(step, which, part):
        block = pieces.at[across if which == 2 else mine, flipped(me, step), :, columns(part)]
        return remote(
            block,
            block,
            fwd_send.at[which, step, part],
            fwd_recv.at[which, step, part],
            me,
            across if which == 1 else twin,
        )

    def forwarded(step, which, part):
        block = pieces.at[
            (twin, across, diagonal)[which], flipped(me, step), :, columns(part)
        ]
        return remote(
            block,
            block,
            fwd_send.at[which, step, part],
            fwd_recv.at[which, step, part],
            me,
            twin,
        )

    def stage_arrive(step, part):
        if step:
            arrival(flipped(me, step), part).wait_recv()
        forward(step, 1, part).start()
        forward(step, 0, part).start()

    def stage_cross(step, part):
        forwarded(step, 1, part).wait_recv()
        forward(step, 2, part).start()

    def core_copy(chunk, part):
        pair = pair_of(chunk)
        return remote(
            partial.at[:, 1 - core, pair, :, narrow(part)],
            from_core.at[:, pair, :, narrow(part)],
            core_send.at[chunk, part],
            core_recv.at[chunk, part],
            me,
            twin,
        )

    def chip_copy(step, part):
        source = flipped(me, step)
        return remote(
            to_chip.at[source, :, narrow(part)],
            from_chip.at[source, :, narrow(part)],
            chip_send.at[step, part],
            chip_recv.at[step, part],
            me,
            across,
        )

    def stage_compute(chunk, _):
        for step in CHUNKS[chunk]:
            for part in range(HALVES):
                forwarded(step, 0, part).wait_recv()
                forwarded(step, 2, part).wait_recv()
        pair = pair_of(chunk)
        blocks = len(CHUNKS[chunk])
        count = GROUP * blocks * capacity
        held = pieces[:, pair, :, pl.ds(0, width)].reshape(count, width)
        both = jnp.dot(held, gate_up[...], preferred_element_type=f32)
        gate_part = both[:, :hidden_width]
        up_part = both[:, hidden_width:]
        hidden = (gate_part / (1.0 + jnp.exp(-gate_part)) * up_part).astype(bf16)
        tail = pieces[:, pair, :, pl.ds(width, wide - width)].reshape(count, wide - width)
        lane = lax.broadcasted_iota(jnp.int32, (count, wide - width), 1)
        weight = jnp.sum(jnp.where(lane == mine, tail.astype(f32), 0.0), axis=1, keepdims=True)
        tile = math.gcd(half, 1024)
        for part in range(HALVES):
            for start in range(part * half, (part + 1) * half, tile):
                outputs = jnp.dot(
                    hidden, down[:, pl.ds(start, tile)], preferred_element_type=f32
                ).astype(bf16)
                partial[:, :, pair, :, pl.ds(start, tile)] = (
                    (outputs.astype(f32) * weight)
                    .astype(bf16)
                    .reshape(2, 2, blocks, capacity, tile)
                )
            core_copy(chunk, part).start()

    def stage_core_sum(chunk, part):
        core_copy(chunk, part).wait_recv()
        pair = pair_of(chunk)
        span = narrow(part)
        to_chip[pair, :, span] = (
            partial[1 - side, core, pair, :, span].astype(f32)
            + from_core[1 - side, pair, :, span].astype(f32)
        ).astype(bf16)

    def stage_chip(step, part):
        chip_copy(step, part).start()

    def return_copy(peer, part):
        return remote(
            final.at[peer, :, narrow(part)],
            returned.at[me, :, narrow(part)],
            ret_send.at[peer, part],
            ret_recv.at[me, part],
            peer,
            mine,
        )

    def return_arrival(peer, part):
        return remote(
            final.at[peer, :, narrow(part)],
            returned.at[peer, :, narrow(part)],
            ret_send.at[peer, part],
            ret_recv.at[peer, part],
            peer,
            mine,
        )

    def stage_final(step, part):
        chip_copy(step, part).wait_recv()
        source = flipped(me, step)
        span = narrow(part)
        total = (
            partial[side, core, source, :, span].astype(f32)
            + from_core[side, source, :, span].astype(f32)
            + from_chip[source, :, span].astype(f32)
        ).astype(bf16)
        if step:
            final[source, :, span] = total
            return_copy(source, part).start()
        else:
            returned[me, :, span] = total

    result_copies = [
        pltpu.make_async_copy(attended, attended_out, output_sem.at[0]),
        pltpu.make_async_copy(expert_out, expert_result, output_sem.at[1]),
    ]

    def attend():
        wait_keys(1)
        length = n * rows
        every_key = all_keys[...].reshape(length, HEAD_WIDTH)
        every_value = all_values[...].reshape(length, HEAD_WIDTH)
        key_pos = lax.broadcasted_iota(jnp.int32, (rows, length), 1)
        query_pos = lax.broadcasted_iota(jnp.int32, (rows, length), 0) + me * rows
        allowed = key_pos <= query_pos
        for head in range(heads):
            span = pl.ds(head * HEAD_WIDTH, HEAD_WIDTH)
            scores = lax.dot_general(
                queries[:, span],
                every_key,
                (((1,), (1,)), ((), ())),
                preferred_element_type=f32,
            ) * (HEAD_WIDTH ** (-0.5))
            key_gate = jnp.concatenate(
                [all_gates[peer, head : head + 1, :] for peer in range(n)], axis=1
            )
            scores = scores + column(gates[head : head + 1, :]) - key_gate
            scores = jnp.where(allowed, scores, NEGATIVE)
            top = jnp.max(scores, axis=1, keepdims=True)
            weights = jnp.where(allowed, jnp.exp(scores - top), 0.0)
            total = jnp.sum(weights, axis=1, keepdims=True)
            mixed = jnp.dot(weights.astype(bf16), every_value, preferred_element_type=f32)
            attended[:, span] = (mixed / total).astype(bf16)
        result_copies[0].start()

    def keys_on(bit, _):
        wait_keys(bit)
        start_keys(bit // 2)

    def weights_in(*_):
        for copy in weight_copies:
            copy.wait()

    stages = (
        stage_arrive, stage_cross, stage_compute, stage_core_sum, stage_chip, stage_final,
        keys_on, weights_in,
    )

    def run(actions):
        for _, kind, number, part in actions:
            stages[kind](number, part)

    start_keys(4)
    for who, actions in itertools.groupby(PLAN, lambda action: action[0]):
        if who == BOTH:
            run(actions)
        else:
            pl.when(inner == who)(functools.partial(run, tuple(actions)))
    attend()

    for step in range(1, n):
        for part in range(HALVES):
            return_arrival(flipped(me, step), part).wait_recv()
    slot_iota = lax.broadcasted_iota(jnp.int32, (rows, slots), 1).astype(f32)
    take = (slot_iota == slot).astype(f32).astype(bf16)
    expert_out[...] = jnp.dot(
        take, returned[...].reshape(slots, width), preferred_element_type=f32
    ).astype(bf16)
    result_copies[1].start()

    for step in range(1, n):
        peer = flipped(me, step)
        for part in range(HALVES):
            dispatch(peer, part).wait_send()
            return_copy(peer, part).wait_send()
    for part in range(HALVES):
        for chunk in range(len(CHUNKS)):
            core_copy(chunk, part).wait_send()
        for step in range(n):
            for which in range(3):
                forward(step, which, part).wait_send()
            chip_copy(step, part).wait_send()
    for bit in bits:
        for others in key_flips(bit):

            @pl.when(sends_keys(bit, others))
            def _():
                for which in range(3):
                    key_send_copy(which, bit, others).wait_send()
    for copy in result_copies:
        copy.wait()


def handed_on(first, second, first_out, second_out, first_held, second_held, taken, given):
    arrays = ((first, first_held, first_out), (second, second_held, second_out))
    takes = [
        pltpu.make_async_copy(source, held, taken.at[index])
        for index, (source, held, _) in enumerate(arrays)
    ]
    gives = [
        pltpu.make_async_copy(held, target, given.at[index])
        for index, (_, held, target) in enumerate(arrays)
    ]
    for copy in takes:
        copy.start()
    for take, give in zip(takes, gives):
        take.wait()
        give.start()
    for copy in gives:
        copy.wait()


def fused(
    queries, keys, values, cum_gates, expert_in, norm_gain, route_group, route_member,
    route_weight, w_gate, w_up, w_down, capacity,
):
    n = lax.axis_size("ep")
    rows, width = expert_in.shape
    hidden_width = w_gate.shape[-1]
    wide = width + 128
    bf16 = jnp.bfloat16
    vmem = pl.BlockSpec(memory_space=pltpu.VMEM)
    anywhere = pl.BlockSpec(memory_space=pl.ANY)
    dma = pltpu.SemaphoreType.DMA
    block = (n, capacity, width)
    inputs = (
        queries, keys, values, cum_gates.T, expert_in, norm_gain.reshape(1, width), route_group.T,
        route_member.T, route_weight.T,
    )
    results = pl.pallas_call(
        functools.partial(fused_kernel, n, capacity),
        out_shape=(
            jax.ShapeDtypeStruct(queries.shape, bf16),
            jax.ShapeDtypeStruct(expert_in.shape, bf16),
        ),
        in_specs=[anywhere] * 12,
        out_specs=(anywhere, anywhere),
        scratch_shapes=[
            *(pltpu.VMEM(array.shape, array.dtype) for array in inputs),
            pltpu.VMEM(queries.shape, bf16),
            pltpu.VMEM(expert_in.shape, bf16),
            dma((len(inputs),)),
            dma((2,)),
            pltpu.VMEM((n, capacity, wide), bf16),
            pltpu.VMEM((GROUP, n, capacity, wide), bf16),
            pltpu.VMEM((width, 2 * hidden_width), bf16),
            pltpu.VMEM((hidden_width, width), bf16),
            pltpu.VMEM((2, 2) + block, bf16),
            pltpu.VMEM((2,) + block, bf16),
            pltpu.VMEM(block, bf16),
            pltpu.VMEM(block, bf16),
            pltpu.VMEM(block, bf16),
            pltpu.VMEM(block, bf16),
            pltpu.VMEM((n,) + keys.shape, bf16),
            pltpu.VMEM((n,) + values.shape, bf16),
            pltpu.VMEM((8, rows), jnp.float32),
            pltpu.VMEM((n, 8, rows), jnp.float32),
            dma((3,)),
            dma((n, HALVES)),
            dma((n, HALVES)),
            dma((3, n, HALVES)),
            dma((3, n, HALVES)),
            dma((len(CHUNKS), HALVES)),
            dma((len(CHUNKS), HALVES)),
            dma((n, HALVES)),
            dma((n, HALVES)),
            dma((n, HALVES)),
            dma((n, HALVES)),
            dma((3, n)),
            dma((3, n)),
        ],
        compiler_params=pltpu.CompilerParams(
            collective_id=0, has_side_effects=True, vmem_limit_bytes=62 * 1024 * 1024
        ),
        name="fused",
    )(
        *inputs, w_gate, w_up, w_down,
    )
    return pl.pallas_call(
        handed_on,
        out_shape=tuple(jax.ShapeDtypeStruct(result.shape, bf16) for result in results),
        in_specs=[anywhere, anywhere],
        out_specs=(anywhere, anywhere),
        scratch_shapes=[
            *(pltpu.VMEM(result.shape, bf16) for result in results),
            dma((2,)),
            dma((2,)),
        ],
        name="handed_on",
    )(*results)


def per_device(
    queries,
    keys,
    values,
    cum_gates,
    expert_in,
    norm_gain,
    route_group,
    route_member,
    route_weight,
    w_gate,
    w_up,
    w_down,
):
    ep_size = lax.axis_size("ep")
    count_rows = expert_in.shape[0]
    capacity = max(2, (3 * count_rows + 2 * ep_size - 1) // (2 * ep_size))
    fits = keys.shape[1] == HEAD_WIDTH and count_rows == queries.shape[0] == HEAD_WIDTH
    if lax.axis_size("tp") == GROUP and ep_size == 8 and capacity % 8 == 0 and fits:
        return fused(
            queries, keys, values, cum_gates, expert_in, norm_gain, route_group, route_member,
            route_weight, w_gate, w_up, w_down, capacity,
        )
    attended = attention_half(queries, keys, values, cum_gates)
    expert_out = expert_half(
        expert_in, norm_gain, route_group, route_member, route_weight, w_gate, w_up, w_down
    )
    return (attended, expert_out)


def solution(mesh):
    return jax.shard_map(
        per_device,
        mesh=mesh,
        in_specs=(
            P("ep", "tp"),
            P("ep", "tp"),
            P("ep", "tp"),
            P("ep", "tp"),
            P(("ep", "tp"), None),
            P(),
            P(("ep", "tp"), None),
            P(("ep", "tp"), None),
            P(("ep", "tp"), None),
            P(("ep", "tp"), None, None),
            P(("ep", "tp"), None, None),
            P(("ep", "tp"), None, None),
        ),
        out_specs=(P("ep", "tp"), P(("ep", "tp"), None)),
        check_vma=False,
    )
```

```python
import functools
import itertools
import math

import jax
import jax.numpy as jnp
from jax import lax
from jax.experimental import pallas as pl
from jax.experimental.pallas import tpu as pltpu
from jax.sharding import PartitionSpec as P

HEAD_WIDTH = 128
GROUP = 4
TOP = 2


OUTER, INNER, BOTH = range(3)
ARRIVE, CROSS, COMPUTE, CORE_SUM, CHIP, FINAL, KEYS, WEIGHTS, ATTEND, DRAIN = range(10)
HALVES = 2
CHUNKS = ((4, 5), (6, 7), (2, 3), (0, 1))
DISPATCH = ((6, 4, 5, 2, 1, 7, 3), (6, 4, 5, 2, 1, 7, 3))
PLAN = (
    (BOTH, ARRIVE, 0, 1),
    (BOTH, ARRIVE, 0, 0),
    (BOTH, ARRIVE, 1, 0),
    (BOTH, ARRIVE, 1, 1),
    (OUTER, ARRIVE, 6, 1),
    (OUTER, ARRIVE, 2, 1),
    (INNER, ARRIVE, 4, 0),
    (INNER, ARRIVE, 4, 1),
    (INNER, ARRIVE, 5, 0),
    (INNER, ARRIVE, 5, 1),
    (INNER, CROSS, 4, 1),
    (BOTH, CROSS, 0, 1),
    (OUTER, CROSS, 1, 0),
    (INNER, ARRIVE, 2, 0),
    (INNER, CROSS, 4, 0),
    (INNER, CROSS, 0, 0),
    (INNER, CROSS, 5, 1),
    (INNER, CROSS, 5, 0),
    (BOTH, ARRIVE, 6, 0),
    (INNER, ARRIVE, 2, 1),
    (INNER, ARRIVE, 6, 1),
    (INNER, WEIGHTS, 0, 0),
    (INNER, COMPUTE, 0, 0),
    (INNER, CROSS, 1, 1),
    (INNER, CORE_SUM, 0, 0),
    (INNER, CROSS, 2, 0),
    (INNER, CROSS, 2, 1),
    (INNER, CHIP, 4, 0),
    (BOTH, ARRIVE, 3, 0),
    (INNER, CROSS, 1, 0),
    (BOTH, ARRIVE, 3, 1),
    (OUTER, CROSS, 0, 0),
    (OUTER, CROSS, 2, 1),
    (OUTER, CROSS, 6, 1),
    (OUTER, ARRIVE, 2, 0),
    (OUTER, CROSS, 1, 1),
    (BOTH, CROSS, 6, 0),
    (OUTER, WEIGHTS, 0, 0),
    (INNER, CORE_SUM, 0, 1),
    (INNER, FINAL, 4, 0),
    (INNER, CROSS, 6, 1),
    (INNER, CHIP, 5, 1),
    (INNER, CHIP, 4, 1),
    (BOTH, COMPUTE, 3, 0),
    (OUTER, ARRIVE, 7, 0),
    (OUTER, CROSS, 3, 1),
    (BOTH, ARRIVE, 7, 1),
    (OUTER, ARRIVE, 4, 0),
    (OUTER, CROSS, 7, 0),
    (OUTER, ARRIVE, 4, 1),
    (OUTER, CROSS, 7, 1),
    (INNER, FINAL, 5, 1),
    (INNER, CHIP, 5, 0),
    (INNER, CROSS, 3, 0),
    (INNER, CROSS, 3, 1),
    (INNER, ARRIVE, 7, 0),
    (INNER, CORE_SUM, 3, 1),
    (INNER, COMPUTE, 2, 0),
    (BOTH, CORE_SUM, 3, 0),
    (OUTER, CROSS, 3, 0),
    (OUTER, ARRIVE, 5, 0),
    (INNER, KEYS, 4, 0),
    (INNER, CORE_SUM, 2, 1),
    (INNER, CROSS, 7, 1),
    (INNER, FINAL, 4, 1),
    (INNER, CHIP, 1, 1),
    (INNER, CHIP, 1, 0),
    (INNER, CROSS, 7, 0),
    (INNER, CORE_SUM, 2, 0),
    (INNER, CHIP, 3, 1),
    (BOTH, COMPUTE, 1, 0),
    (OUTER, ARRIVE, 5, 1),
    (OUTER, CROSS, 2, 0),
    (OUTER, CORE_SUM, 1, 1),
    (BOTH, CORE_SUM, 1, 0),
    (OUTER, CHIP, 6, 0),
    (OUTER, CHIP, 7, 1),
    (OUTER, COMPUTE, 2, 0),
    (OUTER, CORE_SUM, 2, 0),
    (OUTER, CROSS, 5, 1),
    (OUTER, CROSS, 4, 1),
    (OUTER, CROSS, 5, 0),
    (OUTER, CHIP, 6, 1),
    (OUTER, CHIP, 7, 0),
    (OUTER, CROSS, 4, 0),
    (OUTER, FINAL, 6, 0),
    (OUTER, COMPUTE, 0, 0),
    (OUTER, KEYS, 4, 0),
    (OUTER, CORE_SUM, 2, 1),
    (OUTER, CORE_SUM, 0, 1),
    (OUTER, CHIP, 5, 1),
    (OUTER, CORE_SUM, 0, 0),
    (OUTER, FINAL, 6, 1),
    (OUTER, CHIP, 5, 0),
    (OUTER, CHIP, 4, 1),
    (OUTER, FINAL, 7, 1),
    (OUTER, CHIP, 3, 1),
    (OUTER, CHIP, 4, 0),
    (OUTER, CHIP, 1, 0),
    (OUTER, CORE_SUM, 3, 1),
    (OUTER, FINAL, 7, 0),
    (OUTER, FINAL, 5, 1),
    (INNER, FINAL, 1, 1),
    (INNER, CHIP, 3, 0),
    (BOTH, FINAL, 5, 0),
    (OUTER, FINAL, 4, 1),
    (OUTER, CHIP, 2, 0),
    (OUTER, CHIP, 2, 1),
    (OUTER, KEYS, 2, 0),
    (BOTH, FINAL, 3, 1),
    (OUTER, FINAL, 4, 0),
    (OUTER, CHIP, 1, 1),
    (INNER, CHIP, 2, 0),
    (INNER, CORE_SUM, 1, 1),
    (INNER, CHIP, 2, 1),
    (INNER, CHIP, 7, 0),
    (INNER, CHIP, 7, 1),
    (INNER, FINAL, 3, 0),
    (INNER, CHIP, 6, 1),
    (INNER, CHIP, 6, 0),
    (INNER, CHIP, 0, 0),
    (INNER, KEYS, 2, 0),
    (INNER, FINAL, 7, 0),
    (INNER, FINAL, 7, 1),
    (INNER, FINAL, 6, 1),
    (INNER, FINAL, 2, 0),
    (BOTH, FINAL, 1, 0),
    (OUTER, CHIP, 3, 0),
    (OUTER, CHIP, 0, 1),
    (INNER, ATTEND, 0, 0),
    (INNER, FINAL, 6, 0),
    (BOTH, FINAL, 2, 1),
    (OUTER, CHIP, 0, 0),
    (OUTER, FINAL, 2, 0),
    (OUTER, ATTEND, 0, 0),
    (OUTER, FINAL, 3, 0),
    (OUTER, FINAL, 1, 1),
    (INNER, CHIP, 0, 1),
    (BOTH, DRAIN, 0, 0),
    (OUTER, FINAL, 0, 1),
    (BOTH, FINAL, 0, 0),
    (INNER, FINAL, 0, 1),
)


NEGATIVE = -1e30
EPSILON = 1e-06


def group_fold(states, prepared_group, key_piece, value_piece, start_row, all_gates, key_heads):
    query_rows, query_pos, query_gates = prepared_group
    count_queries = query_rows.shape[0]
    head_count = all_gates.shape[1]
    heads_per_group = head_count // key_heads
    piece_rows = key_piece.shape[0]
    rows_per_block = math.gcd(piece_rows, 512)
    score_scale = HEAD_WIDTH ** (-0.5)

    def key_step(step_index, carried):
        running, totals, accumulated = carried
        offset = step_index * rows_per_block
        key_rows = lax.dynamic_slice_in_dim(key_piece, offset, rows_per_block, 0).reshape(
            rows_per_block, key_heads, HEAD_WIDTH
        )
        rows_of_value = lax.dynamic_slice_in_dim(value_piece, offset, rows_per_block, 0).reshape(
            rows_per_block, key_heads, HEAD_WIDTH
        )
        key_gates = lax.dynamic_slice_in_dim(all_gates, offset, rows_per_block, 0)
        key_pos = offset + jnp.arange(rows_per_block, dtype=jnp.int32)
        scores = jnp.einsum(
            "qgrd,kgd->grqk", query_rows, key_rows, preferred_element_type=jnp.float32
        )
        scores = scores.reshape(head_count, count_queries, rows_per_block) * score_scale
        scores = scores + query_gates.T[:, :, None] - key_gates.T[:, None, :]
        allowed = (key_pos[None, :] <= query_pos[:, None])[None]
        scores = jnp.where(allowed, scores, NEGATIVE)
        new_max = jnp.maximum(running, jnp.max(scores, axis=-1))
        weights = jnp.where(allowed, jnp.exp(scores - new_max[..., None]), 0.0)
        factor = jnp.exp(running - new_max)
        totals = totals * factor + jnp.sum(weights, axis=-1)
        inner_product = jnp.einsum(
            "tjub,btl->tjul",
            weights.astype(jnp.bfloat16).reshape(
                key_heads, heads_per_group, count_queries, rows_per_block
            ),
            rows_of_value,
            preferred_element_type=jnp.float32,
        )
        accumulated = accumulated * factor[..., None] + inner_product.reshape(
            head_count, count_queries, HEAD_WIDTH
        )
        return (new_max, totals, accumulated)

    def run_all(carried):
        return lax.fori_loop(0, piece_rows // rows_per_block, key_step, carried)

    def keep_state(carried):
        return carried

    return lax.cond(start_row <= query_pos[-1], run_all, keep_state, states)


def fold_attention(groups, keys, values, all_gates):
    key_heads = keys.shape[1] // HEAD_WIDTH
    head_count = all_gates.shape[1]
    prepared = []
    initial = []
    for query_block, query_pos in groups:
        count_queries = query_block.shape[0]
        prepared.append(
            (
                query_block.reshape(count_queries, key_heads, head_count // key_heads, HEAD_WIDTH),
                query_pos,
                all_gates[query_pos],
            )
        )
        initial.append(
            (
                jnp.full((head_count, count_queries), NEGATIVE, jnp.float32),
                jnp.zeros((head_count, count_queries), jnp.float32),
                jnp.zeros((head_count, count_queries, HEAD_WIDTH), jnp.float32),
            )
        )
    carried = tuple(initial)
    start_row = jnp.int32(0)
    key_piece = lax.all_gather(keys, "ep", axis=0, tiled=True)
    value_piece = lax.all_gather(values, "ep", axis=0, tiled=True)
    finals = tuple(
        (
            group_fold(
                states, prepared_group, key_piece, value_piece, start_row, all_gates, key_heads
            )
            for states, prepared_group in zip(carried, prepared)
        )
    )
    outputs = []
    for running, totals, accumulated in finals:
        result = accumulated / totals[..., None]
        outputs.append(
            jnp.transpose(result, (1, 0, 2))
            .reshape(result.shape[1], head_count * HEAD_WIDTH)
            .astype(jnp.bfloat16)
        )
    return outputs


def attention_half(queries, keys, values, cum_gates):
    count_rows = queries.shape[0]
    head_count = cum_gates.shape[1]
    ep_index = lax.axis_index("ep")
    all_gates = lax.all_gather(cum_gates, "ep", axis=0, tiled=True)
    query_heads = queries.reshape(count_rows, head_count, HEAD_WIDTH)
    positions = ep_index * count_rows + jnp.arange(count_rows, dtype=jnp.int32)
    outputs = fold_attention([(query_heads, positions)], keys, values, all_gates)
    attended = outputs[0]
    return attended


def expert_half(
    expert_in, norm_gain, route_group, route_member, route_weight, w_gate, w_up, w_down
):
    count_rows, model_width = expert_in.shape
    ep_size = lax.axis_size("ep")
    tp_size = lax.axis_size("tp")
    capacity = max(2, (3 * count_rows + 2 * ep_size - 1) // (2 * ep_size))
    floats = expert_in.astype(jnp.float32)
    normed = (
        floats * lax.rsqrt(jnp.mean(floats * floats, axis=-1, keepdims=True) + EPSILON) * norm_gain
    ).astype(jnp.bfloat16)
    members = jnp.arange(GROUP, dtype=jnp.int32)
    mix_weights = jnp.zeros((count_rows, GROUP), jnp.float32)
    for rank_index in range(TOP):
        mix_weights = mix_weights + route_weight[:, rank_index : rank_index + 1] * (
            route_member[:, rank_index : rank_index + 1] == members[None, :]
        ).astype(jnp.float32)
    mix_weights = mix_weights.astype(jnp.bfloat16)
    group_ids = route_group[:, 0]
    group_match = (group_ids[:, None] == jnp.arange(ep_size, dtype=jnp.int32)[None, :]).astype(
        jnp.int32
    )
    rank_within = jnp.sum((jnp.cumsum(group_match, axis=0) - group_match) * group_match, axis=1)
    slot_of_row = group_ids * capacity + rank_within
    row_of_slot = (
        jnp.full((ep_size * capacity,), count_rows, jnp.int32)
        .at[slot_of_row]
        .set(jnp.arange(count_rows, dtype=jnp.int32))
    )
    padded_rows = jnp.concatenate([normed, jnp.zeros((1, model_width), jnp.bfloat16)], axis=0)
    padded_weights = jnp.concatenate([mix_weights, jnp.zeros((1, GROUP), jnp.bfloat16)], axis=0)
    send_rows = padded_rows[row_of_slot].reshape(ep_size, capacity, model_width)
    send_weights = padded_weights[row_of_slot].reshape(ep_size, capacity, GROUP)
    gate_matrix = w_gate[0]
    up_matrix = w_up[0]
    down_matrix = w_down[0]
    arrived_rows = lax.all_to_all(send_rows, "ep", split_axis=0, concat_axis=0, tiled=True)
    arrived_weights = lax.all_to_all(send_weights, "ep", split_axis=0, concat_axis=0, tiled=True)
    sources = arrived_rows.shape[0]
    per_source = arrived_rows.shape[1]
    flat_rows = arrived_rows.reshape(sources * per_source, model_width)
    pieces = lax.all_gather(flat_rows, "tp", axis=0, tiled=True)
    gate_part = jnp.dot(pieces, gate_matrix, preferred_element_type=jnp.float32)
    up_part = jnp.dot(pieces, up_matrix, preferred_element_type=jnp.float32)
    hidden = (jax.nn.silu(gate_part) * up_part).astype(jnp.bfloat16)
    expert_outputs = jnp.dot(hidden, down_matrix, preferred_element_type=jnp.float32).astype(
        jnp.bfloat16
    )
    member_outputs = lax.all_to_all(
        expert_outputs.reshape(tp_size, sources * per_source, model_width),
        "tp",
        split_axis=0,
        concat_axis=0,
        tiled=True,
    )
    flat_weights = arrived_weights.reshape(sources * per_source, GROUP).astype(jnp.float32)
    combined = jnp.zeros((sources * per_source, model_width), jnp.float32)
    for member in range(GROUP):
        combined = combined + flat_weights[:, member : member + 1] * member_outputs[member]
    mixed = combined.astype(jnp.bfloat16).reshape(sources, per_source, model_width)
    returned = lax.all_to_all(mixed, "ep", split_axis=0, concat_axis=0, tiled=True)
    return returned.reshape(ep_size * capacity, model_width)[slot_of_row]


def flipped(index, bits):
    result = index
    place = 1
    while place <= bits:
        if bits & place:
            result = result + place - 2 * place * ((index // place) % 2)
        place = place * 2
    return result


def column_of(rows):
    row_i = lax.broadcasted_iota(jnp.int32, (rows, rows), 0)
    same = row_i == lax.broadcasted_iota(jnp.int32, (rows, rows), 1)

    def column(row):
        return jnp.sum(jnp.where(same, row.astype(jnp.float32), 0.0), axis=1, keepdims=True)

    return column


def slots_of(route_group, capacity):
    f32, bf16 = jnp.float32, jnp.bfloat16
    rows = route_group.shape[1]
    lanes = lax.broadcasted_iota(jnp.int32, (rows, 128), 1)
    row_i = lax.broadcasted_iota(jnp.int32, (rows, rows), 0)
    earlier = (lax.broadcasted_iota(jnp.int32, (rows, rows), 1) < row_i).astype(bf16)
    group = column_of(rows)(route_group[...])
    match = (group == lanes.astype(f32)).astype(f32)
    ranks = jnp.dot(earlier, match.astype(bf16), preferred_element_type=f32)
    rank_within = jnp.sum(ranks * match, axis=1, keepdims=True)
    return group * float(capacity) + rank_within


def fused_kernel(
    n,
    capacity,
    queries_in,
    keys_in,
    values_in,
    gates_in,
    expert_rows,
    gain_in,
    route_group_in,
    route_member_in,
    route_weight_in,
    w_gate,
    w_up,
    w_down,
    attended_out,
    returned_out,
    queries,
    keys,
    values,
    gates,
    expert_in,
    gain,
    route_group,
    route_member,
    route_weight,
    attended,
    input_sem,
    output_sem,
    send,
    pieces,
    gate_up,
    down,
    partial,
    from_core,
    to_chip,
    from_chip,
    final,
    all_keys,
    all_values,
    own_gates,
    all_gates,
    weight_sem,
    disp_send,
    disp_recv,
    fwd_send,
    fwd_recv,
    both_recv,
    core_send,
    core_recv,
    chip_send,
    chip_recv,
    ret_send,
    ret_recv,
    key_send,
    key_recv,
):
    f32, bf16 = jnp.float32, jnp.bfloat16
    rows, width = expert_in.shape
    hidden_width = down.shape[0]
    wide = pieces.shape[-1]
    me = lax.axis_index("ep")
    mine = lax.axis_index("tp")
    core = mine % 2
    side = mine // 2
    twin = flipped(mine, 1)
    across = flipped(mine, 2)
    diagonal = flipped(mine, 3)

    inputs = (
        (route_group_in, route_group),
        (route_member_in, route_member),
        (route_weight_in, route_weight),
        (expert_rows, expert_in),
        (gain_in, gain),
        (keys_in, keys),
        (values_in, values),
        (gates_in, gates),
        (queries_in, queries),
    )
    input_copies = [
        pltpu.make_async_copy(source, target, input_sem.at[index])
        for index, (source, target) in enumerate(inputs)
    ]
    weight_copies = [
        pltpu.make_async_copy(w_gate.at[0], gate_up.at[:, pl.ds(0, hidden_width)], weight_sem.at[0]),
        pltpu.make_async_copy(
            w_up.at[0], gate_up.at[:, pl.ds(hidden_width, hidden_width)], weight_sem.at[1]
        ),
        pltpu.make_async_copy(w_down.at[0], down, weight_sem.at[2]),
    ]
    for copy in input_copies:
        copy.start()

    def has(index, bit):
        return (index // bit) % 2 == 1

    barrier = pltpu.get_barrier_semaphore()

    def remote(source, target, send_sem, recv_sem, ep, tp):
        return pltpu.make_async_remote_copy(
            src_ref=source,
            dst_ref=target,
            send_sem=send_sem,
            recv_sem=recv_sem,
            device_id={"ep": ep, "tp": tp},
            device_id_type=pl.DeviceIdType.MESH,
        )

    for step in range(1, n):
        pl.semaphore_signal(
            barrier,
            inc=1,
            device_id={"ep": flipped(me, step), "tp": mine},
            device_id_type=pl.DeviceIdType.MESH,
        )
    for other in (twin, across):
        pl.semaphore_signal(
            barrier,
            inc=1,
            device_id={"ep": me, "tp": other},
            device_id_type=pl.DeviceIdType.MESH,
        )

    for copy in input_copies[:5]:
        copy.wait()

    lanes = lax.broadcasted_iota(jnp.int32, (rows, 128), 1)
    column = column_of(rows)
    slot = slots_of(route_group, capacity)
    same = lax.broadcasted_iota(jnp.int32, (rows, rows), 0) == lax.broadcasted_iota(
        jnp.int32, (rows, rows), 1
    )
    slot_row = jnp.sum(jnp.where(same, slot, 0.0), axis=0, keepdims=True)
    slots = n * capacity
    place = (
        lax.broadcasted_iota(jnp.int32, (slots, rows), 0).astype(f32) == slot_row
    ).astype(f32).astype(bf16)
    mix = jnp.zeros((rows, 128), f32)
    for rank_index in range(TOP):
        mix = mix + jnp.where(
            column(route_member[rank_index : rank_index + 1, :]) == lanes.astype(f32),
            column(route_weight[rank_index : rank_index + 1, :]),
            0.0,
        )
    floats = expert_in[...].astype(f32)
    scale = lax.rsqrt(jnp.mean(floats * floats, axis=-1, keepdims=True) + EPSILON)
    normed = (floats * scale * gain[...]).astype(bf16)
    send[:, :, pl.ds(0, width)] = (
        jnp.dot(place, normed, preferred_element_type=f32)
        .astype(bf16)
        .reshape(n, capacity, width)
    )
    send[:, :, pl.ds(width, wide - width)] = (
        jnp.dot(place, mix.astype(bf16), preferred_element_type=f32)
        .astype(bf16)
        .reshape(n, capacity, wide - width)
    )
    pl.semaphore_wait(barrier, n + 1)

    half = width // HALVES
    inner = ((me // 2 + 1) // 2) % 2

    def columns(part):
        return pl.ds(part * half, half + (wide - width if part == HALVES - 1 else 0))

    def narrow(part):
        return pl.ds(part * half, half)

    def dispatch(peer, part):
        return remote(
            send.at[peer, :, columns(part)],
            pieces.at[mine, me, :, columns(part)],
            disp_send.at[0],
            disp_recv.at[me, part],
            peer,
            mine,
        )

    def arrival(peer, part):
        return remote(
            send.at[peer, :, columns(part)],
            pieces.at[mine, peer, :, columns(part)],
            disp_send.at[0],
            disp_recv.at[peer, part],
            peer,
            mine,
        )

    def send_rows(order):
        for step in order:
            for part in range(HALVES):
                dispatch(flipped(me, step), part).start()

    if DISPATCH[0] == DISPATCH[1]:
        send_rows(DISPATCH[0])
    else:
        for kind in range(2):
            pl.when(inner == kind)(functools.partial(send_rows, DISPATCH[kind]))
    for copy in weight_copies:
        copy.start()
    pieces[mine, me] = send[me]
    for copy in input_copies[5:]:
        copy.wait()
    heads = gates.shape[0]
    own_gates[pl.ds(0, heads), :] = gates[...]
    for flip in range(1, n):

        @pl.when(jnp.logical_not(has(me, 1 << (flip.bit_length() - 1))))
        def _():
            block = flipped(me, flip)
            all_keys[block] = jnp.zeros_like(all_keys[block])
            all_values[block] = jnp.zeros_like(all_values[block])
            all_gates[block] = jnp.zeros_like(all_gates[block])

    all_gates[me] = own_gates[...]
    all_keys[me] = keys[...]
    all_values[me] = values[...]


    shared = (all_keys, all_values, all_gates)

    bits = [1 << power for power in reversed(range((n - 1).bit_length()))]

    def high(number):
        return 1 << (number.bit_length() - 1)

    def key_send_copy(which, bit, others):
        block = shared[which].at[flipped(me, others)]
        flip = others | bit
        return remote(
            block,
            block,
            key_send.at[which, flip],
            key_recv.at[which, flip],
            flipped(me, bit),
            mine,
        )

    def key_arrival(which, flip):
        block = shared[which].at[flipped(me, flip)]
        return remote(
            block, block, key_send.at[which, flip], key_recv.at[which, flip], me, mine
        )

    def key_flips(bit):
        return [others for others in range(0, n, 2 * bit)]

    def sends_keys(bit, others):
        return has(me, high(others)) if others else jnp.logical_not(has(me, bit))

    def wait_keys(bit):
        for others in key_flips(bit):
            flip = others | bit

            @pl.when(has(me, high(flip)))
            def _():
                for which in range(3):
                    key_arrival(which, flip).wait_recv()

    def start_keys(bit):
        for others in key_flips(bit):

            @pl.when(sends_keys(bit, others))
            def _():
                for which in range(3):
                    key_send_copy(which, bit, others).start()

    def pair_of(chunk):
        steps = CHUNKS[chunk]
        if len(steps) == 1:
            return pl.ds(flipped(me, steps[0]), 1)
        return pl.ds(flipped(me // 2, steps[0] // 2) * 2, 2)

    def chunk_of(step):
        return [step in steps for steps in CHUNKS].index(True)

    def fwd_recv_of(step, which, part):
        return fwd_recv.at[step, part] if which == 1 else both_recv.at[chunk_of(step)]

    def forward(step, which, part):
        block = pieces.at[across if which == 2 else mine, flipped(me, step), :, columns(part)]
        return remote(
            block,
            block,
            fwd_send.at[0],
            fwd_recv_of(step, which, part),
            me,
            across if which == 1 else twin,
        )

    def forwarded(step, which, part):
        block = pieces.at[
            (twin, across, diagonal)[which], flipped(me, step), :, columns(part)
        ]
        return remote(
            block,
            block,
            fwd_send.at[0],
            fwd_recv_of(step, which, part),
            me,
            twin,
        )

    def stage_arrive(step, part):
        if step:
            arrival(flipped(me, step), part).wait_recv()
        forward(step, 1, part).start()
        forward(step, 0, part).start()

    def stage_cross(step, part):
        forwarded(step, 1, part).wait_recv()
        forward(step, 2, part).start()

    def core_copy(chunk, part):
        pair = pair_of(chunk)
        return remote(
            partial.at[:, 1 - core, pair, :, narrow(part)],
            from_core.at[:, pair, :, narrow(part)],
            core_send.at[0],
            core_recv.at[chunk, part],
            me,
            twin,
        )

    def chip_copy(step, part):
        source = flipped(me, step)
        return remote(
            to_chip.at[source, :, narrow(part)],
            from_chip.at[source, :, narrow(part)],
            chip_send.at[0],
            chip_recv.at[step, part],
            me,
            across,
        )

    def stage_compute(chunk, _):
        landed = pieces.at[pl.ds(0, 2), pl.ds(0, len(CHUNKS[chunk]))]
        pltpu.make_async_copy(landed, landed, both_recv.at[chunk]).wait()
        pair = pair_of(chunk)
        blocks = len(CHUNKS[chunk])
        count = GROUP * blocks * capacity
        held = pieces[:, pair, :, pl.ds(0, width)].reshape(count, width)
        both = jnp.dot(held, gate_up[...], preferred_element_type=f32)
        gate_part = both[:, :hidden_width]
        up_part = both[:, hidden_width:]
        hidden = (gate_part / (1.0 + jnp.exp(-gate_part)) * up_part).astype(bf16)
        tail = pieces[:, pair, :, pl.ds(width, wide - width)].reshape(count, wide - width)
        lane = lax.broadcasted_iota(jnp.int32, (count, wide - width), 1)
        weight = jnp.sum(jnp.where(lane == mine, tail.astype(f32), 0.0), axis=1, keepdims=True)
        tile = math.gcd(half, 1024)
        for part in range(HALVES):
            for start in range(part * half, (part + 1) * half, tile):
                outputs = jnp.dot(
                    hidden, down[:, pl.ds(start, tile)], preferred_element_type=f32
                ).astype(bf16)
                partial[:, :, pair, :, pl.ds(start, tile)] = (
                    (outputs.astype(f32) * weight)
                    .astype(bf16)
                    .reshape(2, 2, blocks, capacity, tile)
                )
            core_copy(chunk, part).start()

    def stage_core_sum(chunk, part):
        core_copy(chunk, part).wait_recv()
        pair = pair_of(chunk)
        span = narrow(part)
        to_chip[pair, :, span] = (
            partial[1 - side, core, pair, :, span].astype(f32)
            + from_core[1 - side, pair, :, span].astype(f32)
        ).astype(bf16)

    def stage_chip(step, part):
        chip_copy(step, part).start()

    def return_copy(peer, part):
        return remote(
            final.at[peer, :, narrow(part)],
            returned_out.at[me, :, narrow(part)],
            ret_send.at[0],
            ret_recv.at[0],
            peer,
            mine,
        )

    def own_copy(part):
        return pltpu.make_async_copy(
            final.at[me, :, narrow(part)],
            returned_out.at[me, :, narrow(part)],
            output_sem.at[1 + part],
        )

    def stage_final(step, part):
        chip_copy(step, part).wait_recv()
        source = flipped(me, step)
        span = narrow(part)
        total = (
            partial[side, core, source, :, span].astype(f32)
            + from_core[side, source, :, span].astype(f32)
            + from_chip[source, :, span].astype(f32)
        ).astype(bf16)
        final[source, :, span] = total
        if step:
            return_copy(source, part).start()
        else:
            own_copy(part).start()

    attended_copy = pltpu.make_async_copy(attended, attended_out, output_sem.at[0])

    def attend(*_):
        wait_keys(1)
        length = n * rows
        every_key = all_keys[...].reshape(length, HEAD_WIDTH)
        every_value = all_values[...].reshape(length, HEAD_WIDTH)
        key_pos = lax.broadcasted_iota(jnp.int32, (rows, length), 1)
        query_pos = lax.broadcasted_iota(jnp.int32, (rows, length), 0) + me * rows
        allowed = key_pos <= query_pos
        for head in range(heads):
            span = pl.ds(head * HEAD_WIDTH, HEAD_WIDTH)
            scores = lax.dot_general(
                queries[:, span],
                every_key,
                (((1,), (1,)), ((), ())),
                preferred_element_type=f32,
            ) * (HEAD_WIDTH ** (-0.5))
            key_gate = jnp.concatenate(
                [all_gates[peer, head : head + 1, :] for peer in range(n)], axis=1
            )
            scores = scores + column(gates[head : head + 1, :]) - key_gate
            scores = jnp.where(allowed, scores, NEGATIVE)
            top = jnp.max(scores, axis=1, keepdims=True)
            weights = jnp.where(allowed, jnp.exp(scores - top), 0.0)
            total = jnp.sum(weights, axis=1, keepdims=True)
            mixed = jnp.dot(weights.astype(bf16), every_value, preferred_element_type=f32)
            attended[:, span] = (mixed / total).astype(bf16)
        attended_copy.start()

    def keys_on(bit, _):
        wait_keys(bit)
        start_keys(bit // 2)

    def weights_in(*_):
        for copy in weight_copies:
            copy.wait()

    def drain(*_):
        for held, semaphore in (
            (send.at[pl.ds(1, n - 1)], disp_send),
            (pieces.at[pl.ds(0, 3)], fwd_send),
            (from_core, core_send),
        ):
            pltpu.make_async_copy(held, held, semaphore.at[0]).wait()
        for bit in bits:
            for others in key_flips(bit):

                @pl.when(sends_keys(bit, others))
                def _():
                    for which in range(3):
                        key_send_copy(which, bit, others).wait_send()

    stages = (
        stage_arrive, stage_cross, stage_compute, stage_core_sum, stage_chip, stage_final,
        keys_on, weights_in, attend, drain,
    )

    def run(actions):
        for _, kind, number, part in actions:
            stages[kind](number, part)

    start_keys(4)
    for who, actions in itertools.groupby(PLAN, lambda action: action[0]):
        if who == BOTH:
            run(actions)
        else:
            pl.when(inner == who)(functools.partial(run, tuple(actions)))
    for held, semaphore in (
        (final.at[pl.ds(1, n - 1)], ret_recv),
        (to_chip, chip_send),
        (final.at[pl.ds(1, n - 1)], ret_send),
    ):
        pltpu.make_async_copy(held, held, semaphore.at[0]).wait()
    attended_copy.wait()
    for part in range(HALVES):
        own_copy(part).wait()


def gather_kernel(
    capacity, attended_in, returned_in, route_in, attended_out, expert_result, attended, returned,
    route_group, expert_out, taken, given,
):
    f32, bf16 = jnp.float32, jnp.bfloat16
    slots, width = returned.shape
    rows = expert_out.shape[0]
    tile = math.gcd(width, 1024)
    spans = [pl.ds(start, tile) for start in range(0, width, tile)]
    route = pltpu.make_async_copy(route_in, route_group, taken.at[0])
    takes = [
        pltpu.make_async_copy(returned_in.at[:, span], returned.at[:, span], taken.at[2 + index])
        for index, span in enumerate(spans)
    ]
    gives = [
        pltpu.make_async_copy(
            expert_out.at[:, span], expert_result.at[:, span], given.at[1 + index]
        )
        for index, span in enumerate(spans)
    ]
    attended_take = pltpu.make_async_copy(attended_in, attended, taken.at[1])
    attended_give = pltpu.make_async_copy(attended, attended_out, given.at[0])
    for copy in (route, *takes, attended_take):
        copy.start()
    route.wait()
    slot = slots_of(route_group, capacity)
    slot_iota = lax.broadcasted_iota(jnp.int32, (rows, slots), 1).astype(f32)
    choose = (slot_iota == slot).astype(f32).astype(bf16)
    for span, take, give in zip(spans, takes, gives):
        take.wait()
        expert_out[:, span] = jnp.dot(
            choose, returned[:, span], preferred_element_type=f32
        ).astype(bf16)
        give.start()
    attended_take.wait()
    attended_give.start()
    for copy in (*gives, attended_give):
        copy.wait()


def fused(
    queries, keys, values, cum_gates, expert_in, norm_gain, route_group, route_member,
    route_weight, w_gate, w_up, w_down, capacity,
):
    n = lax.axis_size("ep")
    rows, width = expert_in.shape
    hidden_width = w_gate.shape[-1]
    wide = width + 128
    bf16 = jnp.bfloat16
    vmem = pl.BlockSpec(memory_space=pltpu.VMEM)
    anywhere = pl.BlockSpec(memory_space=pl.ANY)
    dma = pltpu.SemaphoreType.DMA
    block = (n, capacity, width)
    inputs = (
        queries, keys, values, cum_gates.T, expert_in, norm_gain.reshape(1, width), route_group.T,
        route_member.T, route_weight.T,
    )
    attended, returned = pl.pallas_call(
        functools.partial(fused_kernel, n, capacity),
        out_shape=(
            jax.ShapeDtypeStruct(queries.shape, bf16),
            jax.ShapeDtypeStruct(block, bf16),
        ),
        in_specs=[anywhere] * 12,
        out_specs=(anywhere, anywhere),
        scratch_shapes=[
            *(pltpu.VMEM(array.shape, array.dtype) for array in inputs),
            pltpu.VMEM(queries.shape, bf16),
            dma((len(inputs),)),
            dma((1 + HALVES,)),
            pltpu.VMEM((n, capacity, wide), bf16),
            pltpu.VMEM((GROUP, n, capacity, wide), bf16),
            pltpu.VMEM((width, 2 * hidden_width), bf16),
            pltpu.VMEM((hidden_width, width), bf16),
            pltpu.VMEM((2, 2) + block, bf16),
            pltpu.VMEM((2,) + block, bf16),
            pltpu.VMEM(block, bf16),
            pltpu.VMEM(block, bf16),
            pltpu.VMEM(block, bf16),
            pltpu.VMEM((n,) + keys.shape, bf16),
            pltpu.VMEM((n,) + values.shape, bf16),
            pltpu.VMEM((8, rows), jnp.float32),
            pltpu.VMEM((n, 8, rows), jnp.float32),
            dma((3,)),
            dma((1,)),
            dma((n, HALVES)),
            dma((1,)),
            dma((n, HALVES)),
            dma((len(CHUNKS),)),
            dma((1,)),
            dma((len(CHUNKS), HALVES)),
            dma((1,)),
            dma((n, HALVES)),
            dma((1,)),
            dma((1,)),
            dma((3, n)),
            dma((3, n)),
        ],
        compiler_params=pltpu.CompilerParams(
            collective_id=0, has_side_effects=True, vmem_limit_bytes=62 * 1024 * 1024
        ),
        name="fused",
    )(
        *inputs, w_gate, w_up, w_down,
    )
    slots = n * capacity
    tiles = width // math.gcd(width, 1024)
    return pl.pallas_call(
        functools.partial(gather_kernel, capacity),
        out_shape=(
            jax.ShapeDtypeStruct(queries.shape, bf16),
            jax.ShapeDtypeStruct(expert_in.shape, bf16),
        ),
        in_specs=[anywhere] * 3,
        out_specs=(anywhere, anywhere),
        scratch_shapes=[
            pltpu.VMEM(queries.shape, bf16),
            pltpu.VMEM((slots, width), bf16),
            pltpu.VMEM((1, rows), jnp.int32),
            pltpu.VMEM(expert_in.shape, bf16),
            dma((2 + tiles,)),
            dma((1 + tiles,)),
        ],
        name="gathered",
    )(attended, returned.reshape(slots, width), route_group.T)


def per_device(
    queries,
    keys,
    values,
    cum_gates,
    expert_in,
    norm_gain,
    route_group,
    route_member,
    route_weight,
    w_gate,
    w_up,
    w_down,
):
    ep_size = lax.axis_size("ep")
    count_rows = expert_in.shape[0]
    capacity = max(2, (3 * count_rows + 2 * ep_size - 1) // (2 * ep_size))
    fits = keys.shape[1] == HEAD_WIDTH and count_rows == queries.shape[0] == HEAD_WIDTH
    if lax.axis_size("tp") == GROUP and ep_size == 8 and capacity % 8 == 0 and fits:
        return fused(
            queries, keys, values, cum_gates, expert_in, norm_gain, route_group, route_member,
            route_weight, w_gate, w_up, w_down, capacity,
        )
    attended = attention_half(queries, keys, values, cum_gates)
    expert_out = expert_half(
        expert_in, norm_gain, route_group, route_member, route_weight, w_gate, w_up, w_down
    )
    return (attended, expert_out)


def solution(mesh):
    return jax.shard_map(
        per_device,
        mesh=mesh,
        in_specs=(
            P("ep", "tp"),
            P("ep", "tp"),
            P("ep", "tp"),
            P("ep", "tp"),
            P(("ep", "tp"), None),
            P(),
            P(("ep", "tp"), None),
            P(("ep", "tp"), None),
            P(("ep", "tp"), None),
            P(("ep", "tp"), None, None),
            P(("ep", "tp"), None, None),
            P(("ep", "tp"), None, None),
        ),
        out_specs=(P("ep", "tp"), P(("ep", "tp"), None)),
        check_vma=False,
    )
```

```python
import functools
import itertools
import math

import jax
import jax.numpy as jnp
from jax import lax
from jax.experimental import pallas as pl
from jax.experimental.pallas import tpu as pltpu
from jax.sharding import PartitionSpec as P

HEAD_WIDTH = 128
GROUP = 4
TOP = 2


OUTER, INNER, BOTH = range(3)
ARRIVE, CROSS, COMPUTE, CORE_SUM, CHIP, FINAL, KEYS, WEIGHTS, ATTEND, DRAIN = range(10)
HALVES = 2
CHUNKS = ((4, 5), (6, 7), (2, 3), (0, 1))
DISPATCH = ((6, 4, 5, 2, 1, 7, 3), (6, 4, 5, 2, 1, 7, 3))
PLAN = (
    (BOTH, ARRIVE, 0, 1),
    (BOTH, ARRIVE, 0, 0),
    (BOTH, ARRIVE, 1, 0),
    (BOTH, ARRIVE, 1, 1),
    (OUTER, ARRIVE, 6, 1),
    (OUTER, ARRIVE, 2, 1),
    (INNER, ARRIVE, 4, 0),
    (INNER, ARRIVE, 4, 1),
    (INNER, ARRIVE, 5, 0),
    (INNER, ARRIVE, 5, 1),
    (INNER, CROSS, 4, 1),
    (BOTH, CROSS, 0, 1),
    (OUTER, CROSS, 1, 0),
    (INNER, ARRIVE, 2, 0),
    (INNER, CROSS, 4, 0),
    (INNER, CROSS, 0, 0),
    (INNER, CROSS, 5, 1),
    (INNER, CROSS, 5, 0),
    (BOTH, ARRIVE, 6, 0),
    (INNER, ARRIVE, 2, 1),
    (INNER, ARRIVE, 6, 1),
    (INNER, WEIGHTS, 0, 0),
    (INNER, COMPUTE, 0, 0),
    (INNER, CROSS, 1, 1),
    (INNER, CORE_SUM, 0, 0),
    (INNER, CROSS, 2, 0),
    (INNER, CROSS, 2, 1),
    (INNER, CHIP, 4, 0),
    (BOTH, ARRIVE, 3, 0),
    (INNER, CROSS, 1, 0),
    (BOTH, ARRIVE, 3, 1),
    (OUTER, CROSS, 0, 0),
    (OUTER, CROSS, 2, 1),
    (OUTER, CROSS, 6, 1),
    (OUTER, ARRIVE, 2, 0),
    (OUTER, CROSS, 1, 1),
    (BOTH, CROSS, 6, 0),
    (OUTER, WEIGHTS, 0, 0),
    (INNER, CORE_SUM, 0, 1),
    (INNER, FINAL, 4, 0),
    (INNER, CROSS, 6, 1),
    (INNER, CHIP, 5, 1),
    (INNER, CHIP, 4, 1),
    (BOTH, COMPUTE, 3, 0),
    (OUTER, ARRIVE, 7, 0),
    (OUTER, CROSS, 3, 1),
    (BOTH, ARRIVE, 7, 1),
    (OUTER, ARRIVE, 4, 0),
    (OUTER, CROSS, 7, 0),
    (OUTER, ARRIVE, 4, 1),
    (OUTER, CROSS, 7, 1),
    (INNER, FINAL, 5, 1),
    (INNER, CHIP, 5, 0),
    (INNER, CROSS, 3, 0),
    (INNER, CROSS, 3, 1),
    (INNER, ARRIVE, 7, 0),
    (INNER, CORE_SUM, 3, 1),
    (INNER, COMPUTE, 2, 0),
    (BOTH, CORE_SUM, 3, 0),
    (OUTER, CROSS, 3, 0),
    (OUTER, ARRIVE, 5, 0),
    (INNER, KEYS, 4, 0),
    (INNER, CORE_SUM, 2, 1),
    (INNER, CROSS, 7, 1),
    (INNER, FINAL, 4, 1),
    (INNER, CHIP, 1, 1),
    (INNER, CHIP, 1, 0),
    (INNER, CROSS, 7, 0),
    (INNER, CORE_SUM, 2, 0),
    (INNER, CHIP, 3, 1),
    (BOTH, COMPUTE, 1, 0),
    (OUTER, ARRIVE, 5, 1),
    (OUTER, CROSS, 2, 0),
    (OUTER, CORE_SUM, 1, 1),
    (BOTH, CORE_SUM, 1, 0),
    (OUTER, CHIP, 6, 0),
    (OUTER, CHIP, 7, 1),
    (OUTER, COMPUTE, 2, 0),
    (OUTER, CORE_SUM, 2, 0),
    (OUTER, CROSS, 5, 1),
    (OUTER, CROSS, 4, 1),
    (OUTER, CROSS, 5, 0),
    (OUTER, CHIP, 6, 1),
    (OUTER, CHIP, 7, 0),
    (OUTER, CROSS, 4, 0),
    (OUTER, FINAL, 6, 0),
    (OUTER, COMPUTE, 0, 0),
    (OUTER, KEYS, 4, 0),
    (OUTER, CORE_SUM, 2, 1),
    (OUTER, CORE_SUM, 0, 1),
    (OUTER, CHIP, 5, 1),
    (OUTER, CORE_SUM, 0, 0),
    (OUTER, FINAL, 6, 1),
    (OUTER, CHIP, 5, 0),
    (OUTER, CHIP, 4, 1),
    (OUTER, FINAL, 7, 1),
    (OUTER, CHIP, 3, 1),
    (OUTER, CHIP, 4, 0),
    (OUTER, CHIP, 1, 0),
    (OUTER, CORE_SUM, 3, 1),
    (OUTER, FINAL, 7, 0),
    (OUTER, FINAL, 5, 1),
    (INNER, FINAL, 1, 1),
    (INNER, CHIP, 3, 0),
    (BOTH, FINAL, 5, 0),
    (OUTER, FINAL, 4, 1),
    (OUTER, CHIP, 2, 0),
    (OUTER, CHIP, 2, 1),
    (OUTER, KEYS, 2, 0),
    (BOTH, FINAL, 3, 1),
    (OUTER, FINAL, 4, 0),
    (OUTER, CHIP, 3, 0),
    (INNER, CHIP, 2, 0),
    (INNER, CORE_SUM, 1, 1),
    (INNER, CHIP, 2, 1),
    (INNER, CHIP, 7, 0),
    (INNER, CHIP, 7, 1),
    (INNER, FINAL, 3, 0),
    (INNER, CHIP, 6, 1),
    (INNER, CHIP, 6, 0),
    (INNER, CHIP, 0, 0),
    (INNER, KEYS, 2, 0),
    (INNER, FINAL, 7, 0),
    (INNER, FINAL, 7, 1),
    (INNER, FINAL, 6, 1),
    (INNER, FINAL, 2, 0),
    (BOTH, FINAL, 1, 0),
    (OUTER, CHIP, 1, 1),
    (OUTER, CHIP, 0, 1),
    (INNER, ATTEND, 0, 0),
    (INNER, FINAL, 6, 0),
    (BOTH, FINAL, 2, 1),
    (OUTER, CHIP, 0, 0),
    (OUTER, FINAL, 2, 0),
    (OUTER, FINAL, 3, 0),
    (OUTER, ATTEND, 0, 0),
    (OUTER, FINAL, 1, 1),
    (INNER, CHIP, 0, 1),
    (BOTH, DRAIN, 0, 0),
    (OUTER, FINAL, 0, 1),
    (BOTH, FINAL, 0, 0),
    (INNER, FINAL, 0, 1),
)


NEGATIVE = -1e30
EPSILON = 1e-06


def group_fold(states, prepared_group, key_piece, value_piece, start_row, all_gates, key_heads):
    query_rows, query_pos, query_gates = prepared_group
    count_queries = query_rows.shape[0]
    head_count = all_gates.shape[1]
    heads_per_group = head_count // key_heads
    piece_rows = key_piece.shape[0]
    rows_per_block = math.gcd(piece_rows, 512)
    score_scale = HEAD_WIDTH ** (-0.5)

    def key_step(step_index, carried):
        running, totals, accumulated = carried
        offset = step_index * rows_per_block
        key_rows = lax.dynamic_slice_in_dim(key_piece, offset, rows_per_block, 0).reshape(
            rows_per_block, key_heads, HEAD_WIDTH
        )
        rows_of_value = lax.dynamic_slice_in_dim(value_piece, offset, rows_per_block, 0).reshape(
            rows_per_block, key_heads, HEAD_WIDTH
        )
        key_gates = lax.dynamic_slice_in_dim(all_gates, offset, rows_per_block, 0)
        key_pos = offset + jnp.arange(rows_per_block, dtype=jnp.int32)
        scores = jnp.einsum(
            "qgrd,kgd->grqk", query_rows, key_rows, preferred_element_type=jnp.float32
        )
        scores = scores.reshape(head_count, count_queries, rows_per_block) * score_scale
        scores = scores + query_gates.T[:, :, None] - key_gates.T[:, None, :]
        allowed = (key_pos[None, :] <= query_pos[:, None])[None]
        scores = jnp.where(allowed, scores, NEGATIVE)
        new_max = jnp.maximum(running, jnp.max(scores, axis=-1))
        weights = jnp.where(allowed, jnp.exp(scores - new_max[..., None]), 0.0)
        factor = jnp.exp(running - new_max)
        totals = totals * factor + jnp.sum(weights, axis=-1)
        inner_product = jnp.einsum(
            "tjub,btl->tjul",
            weights.astype(jnp.bfloat16).reshape(
                key_heads, heads_per_group, count_queries, rows_per_block
            ),
            rows_of_value,
            preferred_element_type=jnp.float32,
        )
        accumulated = accumulated * factor[..., None] + inner_product.reshape(
            head_count, count_queries, HEAD_WIDTH
        )
        return (new_max, totals, accumulated)

    def run_all(carried):
        return lax.fori_loop(0, piece_rows // rows_per_block, key_step, carried)

    def keep_state(carried):
        return carried

    return lax.cond(start_row <= query_pos[-1], run_all, keep_state, states)


def fold_attention(groups, keys, values, all_gates):
    key_heads = keys.shape[1] // HEAD_WIDTH
    head_count = all_gates.shape[1]
    prepared = []
    initial = []
    for query_block, query_pos in groups:
        count_queries = query_block.shape[0]
        prepared.append(
            (
                query_block.reshape(count_queries, key_heads, head_count // key_heads, HEAD_WIDTH),
                query_pos,
                all_gates[query_pos],
            )
        )
        initial.append(
            (
                jnp.full((head_count, count_queries), NEGATIVE, jnp.float32),
                jnp.zeros((head_count, count_queries), jnp.float32),
                jnp.zeros((head_count, count_queries, HEAD_WIDTH), jnp.float32),
            )
        )
    carried = tuple(initial)
    start_row = jnp.int32(0)
    key_piece = lax.all_gather(keys, "ep", axis=0, tiled=True)
    value_piece = lax.all_gather(values, "ep", axis=0, tiled=True)
    finals = tuple(
        (
            group_fold(
                states, prepared_group, key_piece, value_piece, start_row, all_gates, key_heads
            )
            for states, prepared_group in zip(carried, prepared)
        )
    )
    outputs = []
    for running, totals, accumulated in finals:
        result = accumulated / totals[..., None]
        outputs.append(
            jnp.transpose(result, (1, 0, 2))
            .reshape(result.shape[1], head_count * HEAD_WIDTH)
            .astype(jnp.bfloat16)
        )
    return outputs


def attention_half(queries, keys, values, cum_gates):
    count_rows = queries.shape[0]
    head_count = cum_gates.shape[1]
    ep_index = lax.axis_index("ep")
    all_gates = lax.all_gather(cum_gates, "ep", axis=0, tiled=True)
    query_heads = queries.reshape(count_rows, head_count, HEAD_WIDTH)
    positions = ep_index * count_rows + jnp.arange(count_rows, dtype=jnp.int32)
    outputs = fold_attention([(query_heads, positions)], keys, values, all_gates)
    attended = outputs[0]
    return attended


def expert_half(
    expert_in, norm_gain, route_group, route_member, route_weight, w_gate, w_up, w_down
):
    count_rows, model_width = expert_in.shape
    ep_size = lax.axis_size("ep")
    tp_size = lax.axis_size("tp")
    capacity = max(2, (3 * count_rows + 2 * ep_size - 1) // (2 * ep_size))
    floats = expert_in.astype(jnp.float32)
    normed = (
        floats * lax.rsqrt(jnp.mean(floats * floats, axis=-1, keepdims=True) + EPSILON) * norm_gain
    ).astype(jnp.bfloat16)
    members = jnp.arange(GROUP, dtype=jnp.int32)
    mix_weights = jnp.zeros((count_rows, GROUP), jnp.float32)
    for rank_index in range(TOP):
        mix_weights = mix_weights + route_weight[:, rank_index : rank_index + 1] * (
            route_member[:, rank_index : rank_index + 1] == members[None, :]
        ).astype(jnp.float32)
    mix_weights = mix_weights.astype(jnp.bfloat16)
    group_ids = route_group[:, 0]
    group_match = (group_ids[:, None] == jnp.arange(ep_size, dtype=jnp.int32)[None, :]).astype(
        jnp.int32
    )
    rank_within = jnp.sum((jnp.cumsum(group_match, axis=0) - group_match) * group_match, axis=1)
    slot_of_row = group_ids * capacity + rank_within
    row_of_slot = (
        jnp.full((ep_size * capacity,), count_rows, jnp.int32)
        .at[slot_of_row]
        .set(jnp.arange(count_rows, dtype=jnp.int32))
    )
    padded_rows = jnp.concatenate([normed, jnp.zeros((1, model_width), jnp.bfloat16)], axis=0)
    padded_weights = jnp.concatenate([mix_weights, jnp.zeros((1, GROUP), jnp.bfloat16)], axis=0)
    send_rows = padded_rows[row_of_slot].reshape(ep_size, capacity, model_width)
    send_weights = padded_weights[row_of_slot].reshape(ep_size, capacity, GROUP)
    gate_matrix = w_gate[0]
    up_matrix = w_up[0]
    down_matrix = w_down[0]
    arrived_rows = lax.all_to_all(send_rows, "ep", split_axis=0, concat_axis=0, tiled=True)
    arrived_weights = lax.all_to_all(send_weights, "ep", split_axis=0, concat_axis=0, tiled=True)
    sources = arrived_rows.shape[0]
    per_source = arrived_rows.shape[1]
    flat_rows = arrived_rows.reshape(sources * per_source, model_width)
    pieces = lax.all_gather(flat_rows, "tp", axis=0, tiled=True)
    gate_part = jnp.dot(pieces, gate_matrix, preferred_element_type=jnp.float32)
    up_part = jnp.dot(pieces, up_matrix, preferred_element_type=jnp.float32)
    hidden = (jax.nn.silu(gate_part) * up_part).astype(jnp.bfloat16)
    expert_outputs = jnp.dot(hidden, down_matrix, preferred_element_type=jnp.float32).astype(
        jnp.bfloat16
    )
    member_outputs = lax.all_to_all(
        expert_outputs.reshape(tp_size, sources * per_source, model_width),
        "tp",
        split_axis=0,
        concat_axis=0,
        tiled=True,
    )
    flat_weights = arrived_weights.reshape(sources * per_source, GROUP).astype(jnp.float32)
    combined = jnp.zeros((sources * per_source, model_width), jnp.float32)
    for member in range(GROUP):
        combined = combined + flat_weights[:, member : member + 1] * member_outputs[member]
    mixed = combined.astype(jnp.bfloat16).reshape(sources, per_source, model_width)
    returned = lax.all_to_all(mixed, "ep", split_axis=0, concat_axis=0, tiled=True)
    return returned.reshape(ep_size * capacity, model_width)[slot_of_row]


def flipped(index, bits):
    result = index
    place = 1
    while place <= bits:
        if bits & place:
            result = result + place - 2 * place * ((index // place) % 2)
        place = place * 2
    return result


def column_of(rows):
    row_i = lax.broadcasted_iota(jnp.int32, (rows, rows), 0)
    same = row_i == lax.broadcasted_iota(jnp.int32, (rows, rows), 1)

    def column(row):
        return jnp.sum(jnp.where(same, row.astype(jnp.float32), 0.0), axis=1, keepdims=True)

    return column


def slots_of(route_group, capacity):
    f32, bf16 = jnp.float32, jnp.bfloat16
    rows = route_group.shape[1]
    lanes = lax.broadcasted_iota(jnp.int32, (rows, 128), 1)
    row_i = lax.broadcasted_iota(jnp.int32, (rows, rows), 0)
    earlier = (lax.broadcasted_iota(jnp.int32, (rows, rows), 1) < row_i).astype(bf16)
    group = column_of(rows)(route_group[...])
    match = (group == lanes.astype(f32)).astype(f32)
    ranks = jnp.dot(earlier, match.astype(bf16), preferred_element_type=f32)
    rank_within = jnp.sum(ranks * match, axis=1, keepdims=True)
    return group * float(capacity) + rank_within


def fused_kernel(
    n,
    capacity,
    queries_in,
    keys_in,
    values_in,
    gates_in,
    expert_rows,
    gain_in,
    route_group_in,
    route_member_in,
    route_weight_in,
    w_gate,
    w_up,
    w_down,
    attended_out,
    returned_out,
    queries,
    keys,
    values,
    gates,
    expert_in,
    gain,
    route_group,
    route_member,
    route_weight,
    attended,
    input_sem,
    output_sem,
    send,
    pieces,
    gate_up,
    down,
    partial,
    from_core,
    to_chip,
    from_chip,
    final,
    all_pairs,
    own_gates,
    all_gates,
    weight_sem,
    disp_send,
    disp_recv,
    fwd_send,
    fwd_recv,
    both_recv,
    core_send,
    core_recv,
    chip_send,
    chip_recv,
    ret_send,
    ret_recv,
    key_send,
    key_recv,
):
    f32, bf16 = jnp.float32, jnp.bfloat16
    rows, width = expert_in.shape
    hidden_width = down.shape[0]
    wide = pieces.shape[-1]
    me = lax.axis_index("ep")
    mine = lax.axis_index("tp")
    core = mine % 2
    side = mine // 2
    twin = flipped(mine, 1)
    across = flipped(mine, 2)
    diagonal = flipped(mine, 3)

    inputs = (
        (route_group_in, route_group),
        (route_member_in, route_member),
        (route_weight_in, route_weight),
        (expert_rows, expert_in),
        (gain_in, gain),
        (keys_in, keys),
        (values_in, values),
        (gates_in, gates),
        (queries_in, queries),
    )
    input_copies = [
        pltpu.make_async_copy(source, target, input_sem.at[index])
        for index, (source, target) in enumerate(inputs)
    ]
    weight_copies = [
        pltpu.make_async_copy(w_gate.at[0], gate_up.at[:, pl.ds(0, hidden_width)], weight_sem.at[0]),
        pltpu.make_async_copy(
            w_up.at[0], gate_up.at[:, pl.ds(hidden_width, hidden_width)], weight_sem.at[1]
        ),
        pltpu.make_async_copy(w_down.at[0], down, weight_sem.at[2]),
    ]
    for copy in input_copies:
        copy.start()

    def has(index, bit):
        return (index // bit) % 2 == 1

    barrier = pltpu.get_barrier_semaphore()

    def remote(source, target, send_sem, recv_sem, ep, tp):
        return pltpu.make_async_remote_copy(
            src_ref=source,
            dst_ref=target,
            send_sem=send_sem,
            recv_sem=recv_sem,
            device_id={"ep": ep, "tp": tp},
            device_id_type=pl.DeviceIdType.MESH,
        )

    for step in range(1, n):
        pl.semaphore_signal(
            barrier,
            inc=1,
            device_id={"ep": flipped(me, step), "tp": mine},
            device_id_type=pl.DeviceIdType.MESH,
        )
    for other in (twin, across):
        pl.semaphore_signal(
            barrier,
            inc=1,
            device_id={"ep": me, "tp": other},
            device_id_type=pl.DeviceIdType.MESH,
        )

    for copy in input_copies[:5]:
        copy.wait()

    lanes = lax.broadcasted_iota(jnp.int32, (rows, 128), 1)
    column = column_of(rows)
    slot = slots_of(route_group, capacity)
    same = lax.broadcasted_iota(jnp.int32, (rows, rows), 0) == lax.broadcasted_iota(
        jnp.int32, (rows, rows), 1
    )
    slot_row = jnp.sum(jnp.where(same, slot, 0.0), axis=0, keepdims=True)
    slots = n * capacity
    place = (
        lax.broadcasted_iota(jnp.int32, (slots, rows), 0).astype(f32) == slot_row
    ).astype(f32).astype(bf16)
    mix = jnp.zeros((rows, 128), f32)
    for rank_index in range(TOP):
        mix = mix + jnp.where(
            column(route_member[rank_index : rank_index + 1, :]) == lanes.astype(f32),
            column(route_weight[rank_index : rank_index + 1, :]),
            0.0,
        )
    floats = expert_in[...].astype(f32)
    scale = lax.rsqrt(jnp.mean(floats * floats, axis=-1, keepdims=True) + EPSILON)
    normed = (floats * scale * gain[...]).astype(bf16)
    send[:, :, pl.ds(0, width)] = (
        jnp.dot(place, normed, preferred_element_type=f32)
        .astype(bf16)
        .reshape(n, capacity, width)
    )
    send[:, :, pl.ds(width, wide - width)] = (
        jnp.dot(place, mix.astype(bf16), preferred_element_type=f32)
        .astype(bf16)
        .reshape(n, capacity, wide - width)
    )
    pl.semaphore_wait(barrier, n + 1)

    half = width // HALVES
    inner = ((me // 2 + 1) // 2) % 2

    def columns(part):
        return pl.ds(part * half, half + (wide - width if part == HALVES - 1 else 0))

    def narrow(part):
        return pl.ds(part * half, half)

    def dispatch(peer, part):
        return remote(
            send.at[peer, :, columns(part)],
            pieces.at[mine, me, :, columns(part)],
            disp_send.at[0],
            disp_recv.at[me, part],
            peer,
            mine,
        )

    def arrival(peer, part):
        return remote(
            send.at[peer, :, columns(part)],
            pieces.at[mine, peer, :, columns(part)],
            disp_send.at[0],
            disp_recv.at[peer, part],
            peer,
            mine,
        )

    def send_rows(order):
        for step in order:
            for part in range(HALVES):
                dispatch(flipped(me, step), part).start()

    if DISPATCH[0] == DISPATCH[1]:
        send_rows(DISPATCH[0])
    else:
        for kind in range(2):
            pl.when(inner == kind)(functools.partial(send_rows, DISPATCH[kind]))
    for copy in weight_copies:
        copy.start()
    pieces[mine, me] = send[me]
    for copy in input_copies[5:]:
        copy.wait()
    heads = gates.shape[0]
    own_gates[pl.ds(0, heads), :] = gates[...]
    for flip in range(1, n):

        @pl.when(jnp.logical_not(has(me, 1 << (flip.bit_length() - 1))))
        def _():
            block = flipped(me, flip)
            all_pairs[block] = jnp.zeros_like(all_pairs[block])
            all_gates[block] = jnp.zeros_like(all_gates[block])

    all_gates[me] = own_gates[...]
    all_pairs[me, pl.ds(0, rows), :] = keys[...]
    all_pairs[me, pl.ds(rows, rows), :] = values[...]


    shared = (all_pairs, all_gates)

    bits = [1 << power for power in reversed(range((n - 1).bit_length()))]

    def high(number):
        return 1 << (number.bit_length() - 1)

    def key_send_copy(which, bit, others):
        block = shared[which].at[flipped(me, others)]
        flip = others | bit
        return remote(
            block,
            block,
            key_send.at[which, flip],
            key_recv.at[which, flip],
            flipped(me, bit),
            mine,
        )

    def key_arrival(which, flip):
        block = shared[which].at[flipped(me, flip)]
        return remote(
            block, block, key_send.at[which, flip], key_recv.at[which, flip], me, mine
        )

    def key_flips(bit):
        return [others for others in range(0, n, 2 * bit)]

    def sends_keys(bit, others):
        return has(me, high(others)) if others else jnp.logical_not(has(me, bit))

    def wait_keys(bit):
        for others in key_flips(bit):
            flip = others | bit

            @pl.when(has(me, high(flip)))
            def _():
                for which in range(2):
                    key_arrival(which, flip).wait_recv()

    def start_keys(bit):
        for others in key_flips(bit):

            @pl.when(sends_keys(bit, others))
            def _():
                for which in range(2):
                    key_send_copy(which, bit, others).start()

    def pair_of(chunk):
        steps = CHUNKS[chunk]
        if len(steps) == 1:
            return pl.ds(flipped(me, steps[0]), 1)
        return pl.ds(flipped(me // 2, steps[0] // 2) * 2, 2)

    def chunk_of(step):
        return [step in steps for steps in CHUNKS].index(True)

    def fwd_recv_of(step, which, part):
        return fwd_recv.at[step, part] if which == 1 else both_recv.at[chunk_of(step)]

    def forward(step, which, part):
        block = pieces.at[across if which == 2 else mine, flipped(me, step), :, columns(part)]
        return remote(
            block,
            block,
            fwd_send.at[0],
            fwd_recv_of(step, which, part),
            me,
            across if which == 1 else twin,
        )

    def forwarded(step, which, part):
        block = pieces.at[
            (twin, across, diagonal)[which], flipped(me, step), :, columns(part)
        ]
        return remote(
            block,
            block,
            fwd_send.at[0],
            fwd_recv_of(step, which, part),
            me,
            twin,
        )

    def stage_arrive(step, part):
        if step:
            arrival(flipped(me, step), part).wait_recv()
        forward(step, 1, part).start()
        forward(step, 0, part).start()

    def stage_cross(step, part):
        forwarded(step, 1, part).wait_recv()
        forward(step, 2, part).start()

    def core_copy(chunk, part):
        pair = pair_of(chunk)
        return remote(
            partial.at[:, 1 - core, pair, :, narrow(part)],
            from_core.at[:, pair, :, narrow(part)],
            core_send.at[0],
            core_recv.at[chunk, part],
            me,
            twin,
        )

    def chip_copy(step, part):
        source = flipped(me, step)
        return remote(
            to_chip.at[source, :, narrow(part)],
            from_chip.at[source, :, narrow(part)],
            chip_send.at[0],
            chip_recv.at[step, part],
            me,
            across,
        )

    def stage_compute(chunk, _):
        landed = pieces.at[pl.ds(0, 2), pl.ds(0, len(CHUNKS[chunk]))]
        pltpu.make_async_copy(landed, landed, both_recv.at[chunk]).wait()
        pair = pair_of(chunk)
        blocks = len(CHUNKS[chunk])
        count = GROUP * blocks * capacity
        held = pieces[:, pair, :, pl.ds(0, width)].reshape(count, width)
        both = jnp.dot(held, gate_up[...], preferred_element_type=f32)
        gate_part = both[:, :hidden_width]
        up_part = both[:, hidden_width:]
        hidden = (gate_part / (1.0 + jnp.exp(-gate_part)) * up_part).astype(bf16)
        tail = pieces[:, pair, :, pl.ds(width, wide - width)].reshape(count, wide - width)
        lane = lax.broadcasted_iota(jnp.int32, (count, wide - width), 1)
        weight = jnp.sum(jnp.where(lane == mine, tail.astype(f32), 0.0), axis=1, keepdims=True)
        tile = math.gcd(half, 1024)
        for part in range(HALVES):
            for start in range(part * half, (part + 1) * half, tile):
                outputs = jnp.dot(
                    hidden, down[:, pl.ds(start, tile)], preferred_element_type=f32
                ).astype(bf16)
                partial[:, :, pair, :, pl.ds(start, tile)] = (
                    (outputs.astype(f32) * weight)
                    .astype(bf16)
                    .reshape(2, 2, blocks, capacity, tile)
                )
            core_copy(chunk, part).start()

    def stage_core_sum(chunk, part):
        core_copy(chunk, part).wait_recv()
        pair = pair_of(chunk)
        span = narrow(part)
        to_chip[pair, :, span] = (
            partial[1 - side, core, pair, :, span].astype(f32)
            + from_core[1 - side, pair, :, span].astype(f32)
        ).astype(bf16)

    def stage_chip(step, part):
        chip_copy(step, part).start()

    def return_copy(peer, part):
        return remote(
            final.at[peer, :, narrow(part)],
            returned_out.at[me, :, narrow(part)],
            ret_send.at[0],
            ret_recv.at[0],
            peer,
            mine,
        )

    def own_copy(part):
        return pltpu.make_async_copy(
            final.at[me, :, narrow(part)],
            returned_out.at[me, :, narrow(part)],
            output_sem.at[1 + part],
        )

    def stage_final(step, part):
        chip_copy(step, part).wait_recv()
        source = flipped(me, step)
        span = narrow(part)
        total = (
            partial[side, core, source, :, span].astype(f32)
            + from_core[side, source, :, span].astype(f32)
            + from_chip[source, :, span].astype(f32)
        ).astype(bf16)
        final[source, :, span] = total
        if step:
            return_copy(source, part).start()
        else:
            own_copy(part).start()

    attended_copy = pltpu.make_async_copy(attended, attended_out, output_sem.at[0])

    def attend(*_):
        wait_keys(1)
        length = n * rows
        every_key = all_pairs[:, pl.ds(0, rows), :].reshape(length, HEAD_WIDTH)
        every_value = all_pairs[:, pl.ds(rows, rows), :].reshape(length, HEAD_WIDTH)
        key_pos = lax.broadcasted_iota(jnp.int32, (rows, length), 1)
        query_pos = lax.broadcasted_iota(jnp.int32, (rows, length), 0) + me * rows
        allowed = key_pos <= query_pos
        for head in range(heads):
            span = pl.ds(head * HEAD_WIDTH, HEAD_WIDTH)
            scores = lax.dot_general(
                queries[:, span],
                every_key,
                (((1,), (1,)), ((), ())),
                preferred_element_type=f32,
            ) * (HEAD_WIDTH ** (-0.5))
            key_gate = jnp.concatenate(
                [all_gates[peer, head : head + 1, :] for peer in range(n)], axis=1
            )
            scores = scores + column(gates[head : head + 1, :]) - key_gate
            scores = jnp.where(allowed, scores, NEGATIVE)
            top = jnp.max(scores, axis=1, keepdims=True)
            weights = jnp.where(allowed, jnp.exp(scores - top), 0.0)
            total = jnp.sum(weights, axis=1, keepdims=True)
            mixed = jnp.dot(weights.astype(bf16), every_value, preferred_element_type=f32)
            attended[:, span] = (mixed / total).astype(bf16)
        attended_copy.start()

    def keys_on(bit, _):
        wait_keys(bit)
        start_keys(bit // 2)

    def weights_in(*_):
        for copy in weight_copies:
            copy.wait()

    def drain(*_):
        for held, semaphore in (
            (send.at[pl.ds(1, n - 1)], disp_send),
            (pieces.at[pl.ds(0, 3)], fwd_send),
            (from_core, core_send),
        ):
            pltpu.make_async_copy(held, held, semaphore.at[0]).wait()
        for bit in bits:
            for others in key_flips(bit):

                @pl.when(sends_keys(bit, others))
                def _():
                    for which in range(2):
                        key_send_copy(which, bit, others).wait_send()

    stages = (
        stage_arrive, stage_cross, stage_compute, stage_core_sum, stage_chip, stage_final,
        keys_on, weights_in, attend, drain,
    )

    def run(actions):
        for _, kind, number, part in actions:
            stages[kind](number, part)

    start_keys(4)
    for who, actions in itertools.groupby(PLAN, lambda action: action[0]):
        if who == BOTH:
            run(actions)
        else:
            pl.when(inner == who)(functools.partial(run, tuple(actions)))
    for held, semaphore in (
        (final.at[pl.ds(1, n - 1)], ret_recv),
        (to_chip, chip_send),
        (final.at[pl.ds(1, n - 1)], ret_send),
    ):
        pltpu.make_async_copy(held, held, semaphore.at[0]).wait()
    attended_copy.wait()
    for part in range(HALVES):
        own_copy(part).wait()


def gather_kernel(
    capacity, attended_in, returned_in, route_in, attended_out, expert_result, attended, returned,
    route_group, expert_out, taken, given,
):
    f32, bf16 = jnp.float32, jnp.bfloat16
    slots, width = returned.shape
    rows = expert_out.shape[0]
    tile = math.gcd(width, 1024)
    spans = [pl.ds(start, tile) for start in range(0, width, tile)]
    route = pltpu.make_async_copy(route_in, route_group, taken.at[0])
    takes = [
        pltpu.make_async_copy(returned_in.at[:, span], returned.at[:, span], taken.at[2 + index])
        for index, span in enumerate(spans)
    ]
    gives = [
        pltpu.make_async_copy(
            expert_out.at[:, span], expert_result.at[:, span], given.at[1 + index]
        )
        for index, span in enumerate(spans)
    ]
    attended_take = pltpu.make_async_copy(attended_in, attended, taken.at[1])
    attended_give = pltpu.make_async_copy(attended, attended_out, given.at[0])
    for copy in (route, *takes, attended_take):
        copy.start()
    route.wait()
    slot = slots_of(route_group, capacity)
    slot_iota = lax.broadcasted_iota(jnp.int32, (rows, slots), 1).astype(f32)
    choose = (slot_iota == slot).astype(f32).astype(bf16)
    for span, take, give in zip(spans, takes, gives):
        take.wait()
        expert_out[:, span] = jnp.dot(
            choose, returned[:, span], preferred_element_type=f32
        ).astype(bf16)
        give.start()
    attended_take.wait()
    attended_give.start()
    for copy in (*gives, attended_give):
        copy.wait()


def fused(
    queries, keys, values, cum_gates, expert_in, norm_gain, route_group, route_member,
    route_weight, w_gate, w_up, w_down, capacity,
):
    n = lax.axis_size("ep")
    rows, width = expert_in.shape
    hidden_width = w_gate.shape[-1]
    wide = width + 128
    bf16 = jnp.bfloat16
    vmem = pl.BlockSpec(memory_space=pltpu.VMEM)
    anywhere = pl.BlockSpec(memory_space=pl.ANY)
    dma = pltpu.SemaphoreType.DMA
    block = (n, capacity, width)
    inputs = (
        queries, keys, values, cum_gates.T, expert_in, norm_gain.reshape(1, width), route_group.T,
        route_member.T, route_weight.T,
    )
    attended, returned = pl.pallas_call(
        functools.partial(fused_kernel, n, capacity),
        out_shape=(
            jax.ShapeDtypeStruct(queries.shape, bf16),
            jax.ShapeDtypeStruct(block, bf16),
        ),
        in_specs=[anywhere] * 12,
        out_specs=(anywhere, anywhere),
        scratch_shapes=[
            *(pltpu.VMEM(array.shape, array.dtype) for array in inputs),
            pltpu.VMEM(queries.shape, bf16),
            dma((len(inputs),)),
            dma((1 + HALVES,)),
            pltpu.VMEM((n, capacity, wide), bf16),
            pltpu.VMEM((GROUP, n, capacity, wide), bf16),
            pltpu.VMEM((width, 2 * hidden_width), bf16),
            pltpu.VMEM((hidden_width, width), bf16),
            pltpu.VMEM((2, 2) + block, bf16),
            pltpu.VMEM((2,) + block, bf16),
            pltpu.VMEM(block, bf16),
            pltpu.VMEM(block, bf16),
            pltpu.VMEM(block, bf16),
            pltpu.VMEM((n, 2 * rows, keys.shape[1]), bf16),
            pltpu.VMEM((8, rows), jnp.float32),
            pltpu.VMEM((n, 8, rows), jnp.float32),
            dma((3,)),
            dma((1,)),
            dma((n, HALVES)),
            dma((1,)),
            dma((n, HALVES)),
            dma((len(CHUNKS),)),
            dma((1,)),
            dma((len(CHUNKS), HALVES)),
            dma((1,)),
            dma((n, HALVES)),
            dma((1,)),
            dma((1,)),
            dma((2, n)),
            dma((2, n)),
        ],
        compiler_params=pltpu.CompilerParams(
            collective_id=0, has_side_effects=True, vmem_limit_bytes=62 * 1024 * 1024
        ),
        name="fused",
    )(
        *inputs, w_gate, w_up, w_down,
    )
    slots = n * capacity
    tiles = width // math.gcd(width, 1024)
    return pl.pallas_call(
        functools.partial(gather_kernel, capacity),
        out_shape=(
            jax.ShapeDtypeStruct(queries.shape, bf16),
            jax.ShapeDtypeStruct(expert_in.shape, bf16),
        ),
        in_specs=[anywhere] * 3,
        out_specs=(anywhere, anywhere),
        scratch_shapes=[
            pltpu.VMEM(queries.shape, bf16),
            pltpu.VMEM((slots, width), bf16),
            pltpu.VMEM((1, rows), jnp.int32),
            pltpu.VMEM(expert_in.shape, bf16),
            dma((2 + tiles,)),
            dma((1 + tiles,)),
        ],
        name="gathered",
    )(attended, returned.reshape(slots, width), route_group.T)


def per_device(
    queries,
    keys,
    values,
    cum_gates,
    expert_in,
    norm_gain,
    route_group,
    route_member,
    route_weight,
    w_gate,
    w_up,
    w_down,
):
    ep_size = lax.axis_size("ep")
    count_rows = expert_in.shape[0]
    capacity = max(2, (3 * count_rows + 2 * ep_size - 1) // (2 * ep_size))
    fits = keys.shape[1] == HEAD_WIDTH and count_rows == queries.shape[0] == HEAD_WIDTH
    if lax.axis_size("tp") == GROUP and ep_size == 8 and capacity % 8 == 0 and fits:
        return fused(
            queries, keys, values, cum_gates, expert_in, norm_gain, route_group, route_member,
            route_weight, w_gate, w_up, w_down, capacity,
        )
    attended = attention_half(queries, keys, values, cum_gates)
    expert_out = expert_half(
        expert_in, norm_gain, route_group, route_member, route_weight, w_gate, w_up, w_down
    )
    return (attended, expert_out)


def solution(mesh):
    return jax.shard_map(
        per_device,
        mesh=mesh,
        in_specs=(
            P("ep", "tp"),
            P("ep", "tp"),
            P("ep", "tp"),
            P("ep", "tp"),
            P(("ep", "tp"), None),
            P(),
            P(("ep", "tp"), None),
            P(("ep", "tp"), None),
            P(("ep", "tp"), None),
            P(("ep", "tp"), None, None),
            P(("ep", "tp"), None, None),
            P(("ep", "tp"), None, None),
        ),
        out_specs=(P("ep", "tp"), P(("ep", "tp"), None)),
        check_vma=False,
    )
```
